512 devices in a mesh: fs: 16 (over z), rep: 4 (over y), tp: 8 (over x, core).
Axes of the slice: x: 4, y: 4, z: 16, core: 2. Of those that a mesh axis runs over, the one named last changes fastest.
Arguments:
- normed_input: bfloat16 [8192, 1024], P(('fs', 'rep')), may hold values from -6 to 6
- query_cotangent: bfloat16 [8192, 512], P(('fs', 'rep'), 'tp'), may hold values from -0.029907227 to 0.029907227
- value_cotangent: bfloat16 [8192, 1024], P(('fs', 'rep'), 'tp'), may hold values from -0.029907227 to 0.029907227
- query_basis: bfloat16 [1024, 128], replicated, may hold values from -0.1875 to 0.1875
- value_basis: bfloat16 [1024, 128], replicated, may hold values from -0.1875 to 0.1875
- query_weight: float32 [1024, 512], P(('fs', 'rep'), 'tp'), may hold values from -0.1875 to 0.1875
- value_weight: float32 [1024, 1024], P(('fs', 'rep'), 'tp'), may hold values from -0.1875 to 0.1875
- query_first: float32 [128, 512], P(('fs', 'rep'), 'tp'), may hold values from -6 to 6
- query_second: float32 [128, 512], P(('fs', 'rep'), 'tp'), may hold values from 0.25 to 4
- value_first: float32 [128, 1024], P(('fs', 'rep'), 'tp'), may hold values from -6 to 6
- value_second: float32 [128, 1024], P(('fs', 'rep'), 'tp'), may hold values from 0.25 to 4
Outputs:
- query_update: float32 [1024, 512], P(('fs', 'rep'), 'tp')
- value_update: float32 [1024, 1024], P(('fs', 'rep'), 'tp')
- query_weight_new: float32 [1024, 512], P(('fs', 'rep'), 'tp')
- value_weight_new: float32 [1024, 1024], P(('fs', 'rep'), 'tp')
- query_first_new: float32 [128, 512], P(('fs', 'rep'), 'tp')
- query_second_new: float32 [128, 512], P(('fs', 'rep'), 'tp')
- value_first_new: float32 [128, 1024], P(('fs', 'rep'), 'tp')
- value_second_new: float32 [128, 1024], P(('fs', 'rep'), 'tp')
- query_copy: bfloat16 [1024, 512], P(None, 'tp')
- value_copy: bfloat16 [1024, 1024], P(None, 'tp')
The draws below stay inside these ranges and needn't reach their ends.
All inputs are finite; a program needn't handle non-finite values.
Results may differ from the reference program's by a relative error of at most 0.001.
Values may be sent and summed in bfloat16 or wider, within the bound.
A program may use at most 64 MiB of HBM per device.

```python
import math
import jax
import jax.numpy as jnp
from jax import lax

D = 1024
RANK = 128
QW = 512
VW = 1024
TOKENS = 8192


def block_levels(stream_key, shape, shards, smallest, top_value):
    gain = 1.0
    for dim, parts in shards:
        steps = jax.random.uniform(jax.random.fold_in(jax.random.fold_in(stream_key, 6), dim), (parts,), jnp.float32, smallest / len(shards), top_value / len(shards))
        gain = gain * jnp.repeat(jnp.exp(steps), shape[dim] // parts).reshape((-1,) + (1,) * (len(shape) - 1 - dim))
    return gain


def normal_values(key, extent, width, most, split=(), dtype=jnp.bfloat16):
    values = jax.random.normal(key, extent, jnp.float32) * width
    if len(split) > 0:
        values = block_levels(key, extent, split, -0.22, 0.18) * values
    return jnp.clip(values, min=-most, max=most).astype(dtype)


def setup_inputs(seed: int = 0) -> dict:
    arg_keys = jax.random.split(jax.random.key(seed), 12)
    normed_input = normal_values(arg_keys[0], (TOKENS, D), 1.0, 6.0, ((0, 64),))
    query_cotangent = normal_values(arg_keys[1], (TOKENS, QW), 0.005, 0.029907227, ((0, 64), (1, 8)))
    value_cotangent = normal_values(arg_keys[2], (TOKENS, VW), 0.005, 0.029907227, ((0, 64), (1, 8)))
    query_basis = normal_values(arg_keys[3], (D, RANK), D ** -0.5, 0.1875)
    value_basis = normal_values(arg_keys[4], (D, RANK), D ** -0.5, 0.1875)
    query_weight = normal_values(arg_keys[5], (D, QW), D ** -0.5, 0.1875, ((0, 64), (1, 8)), jnp.float32)
    value_weight = normal_values(arg_keys[6], (D, VW), D ** -0.5, 0.1875, ((0, 64), (1, 8)), jnp.float32)
    query_first = normal_values(arg_keys[7], (RANK, QW), 1.0, 6.0, ((0, 64), (1, 8)), jnp.float32)
    query_second = jnp.clip(jnp.exp(math.log(4.0) - 2.7725887 * jax.random.uniform(arg_keys[8], (RANK, QW), jnp.float32) ** block_levels(arg_keys[8], (RANK, QW), ((0, 64), (1, 8)), -0.2, 0.2)), 0.25, 4.0)
    value_first = normal_values(arg_keys[9], (RANK, VW), 1.0, 6.0, ((0, 64), (1, 8)), jnp.float32)
    value_second = jnp.clip(jnp.exp(math.log(4.0) - 2.7725887 * jax.random.uniform(arg_keys[10], (RANK, VW), jnp.float32) ** block_levels(arg_keys[10], (RANK, VW), ((0, 64), (1, 8)), -0.2, 0.2)), 0.25, 4.0)
    return dict(normed_input=normed_input, query_cotangent=query_cotangent, value_cotangent=value_cotangent, query_basis=query_basis, value_basis=value_basis, query_weight=query_weight, value_weight=value_weight, query_first=query_first, query_second=query_second, value_first=value_first, value_second=value_second)


def update_matrix(normed_input, cotangent, basis, weight, first_old, second_old):
    gradient = jnp.dot(normed_input.T, cotangent, preferred_element_type=jnp.float32)
    basis_wide = basis.astype(jnp.float32)
    projected = jnp.dot(basis_wide.T, gradient, precision=lax.Precision.HIGHEST)
    first_new = 0.9 * first_old + 0.1 * projected
    second_new = 0.99 * second_old + 0.01 * projected * projected
    direction = first_new / (jnp.sqrt(second_new) + 1e-08)
    norm_scale = jnp.sqrt(jnp.mean(direction * direction) + 1.0)
    update = jnp.dot(basis_wide, direction, precision=lax.Precision.HIGHEST) / norm_scale
    weight_new = weight - 0.01 * update
    return (update, weight_new, first_new, second_new, weight_new.astype(jnp.bfloat16))

def reference(normed_input, query_cotangent, value_cotangent, query_basis, value_basis, query_weight, value_weight, query_first, query_second, value_first, value_second):
    query_out = update_matrix(normed_input, query_cotangent, query_basis, query_weight, query_first, query_second)
    value_out = update_matrix(normed_input, value_cotangent, value_basis, value_weight, value_first, value_second)
    return (query_out[0], value_out[0], query_out[1], value_out[1], query_out[2], query_out[3], value_out[2], value_out[3], query_out[4], value_out[4])
```

```python
import functools

import jax
import jax.numpy as jnp
from jax import lax
from jax.experimental import pallas as pl
from jax.experimental.pallas import tpu as pltpu
from jax.sharding import PartitionSpec as P

F32 = jnp.float32
BF16 = jnp.bfloat16
MESH = pl.DeviceIdType.MESH

Z, Y, T = 16, 4, 8
D, RANK = 1024, 128
QL, VL = 64, 128
ROWS = 16
NEAR = (1, -1, 2, -2, 3, -3, 4, -4)
FAR = (8, 7, 9, 6, 10, 5, 11, 4, 12, 3, 13, 2, 14, 1, 15)
SPLIT_GREETING = True


def query_order(p):
    return p >> 6, (p >> 2) & 15, p & 3


def value_order(p):
    return (p >> 2) & 1, p >> 3, p & 3


def rank_of(order, p):
    h, c, i = order(p)
    return 32 * (2 * h + (i >> 1)) + 8 * (c & 3) + 2 * (c >> 2) + (i & 1)


def iota(shape, dim):
    return lax.broadcasted_iota(jnp.int32, shape, dim)


def one_hot(match):
    return jnp.where(match, 1.0, 0.0).astype(F32).astype(BF16)


def nt(a, b):
    return lax.dot_general(a, b, (((1,), (1,)), ((), ())), preferred_element_type=F32)


def nn(a, b):
    return jnp.dot(a, b, preferred_element_type=F32)


def two_parts(value):
    high = value.astype(BF16)
    return high, (value - high.astype(F32)).astype(BF16)


def exchange(
    x_h, cq_h, cv_h, bq_h, bv_h, wq_h, wv_h, fq_h, sq_h, fv_h, sv_h,
    uv_o, uqt_o, uq_o, wv_o, wqt_o, mom_o, tp_o,
    x, cq, cv, bases, wq, wv, olds_q, olds_v,
    gathered, old, part, from_y, chunk, from_z, old_first, old_second, send_ag, from_ag,
    bq2, bv2, dv, dqp, wqn, squares,
    lsem, ysend, yrecv, zsend, zrecv, nsend, nrecv, rsend, rrecv, wsend, wrecv, osend, orecv,
    asend, arecv, tsend, trecv, greet,
):
    z, y, t = lax.axis_index("fs"), lax.axis_index("rep"), lax.axis_index("tp")
    a = lax.rem(z, 4)
    b = lax.div(z, 4)

    def at_z(k):
        return lax.rem(z + (k % Z), Z)

    def at_y(k):
        return lax.rem(y + (k % Y), Y)

    def at_t(k):
        return lax.rem(t + (k % T), T)

    def where(zz, yy, tt):
        return (zz, yy, tt)

    def remote(src, dst, send, recv, device):
        return pltpu.make_async_remote_copy(
            src_ref=src, dst_ref=dst, send_sem=send, recv_sem=recv, device_id=device, device_id_type=MESH
        )

    barrier = pltpu.get_barrier_semaphore()
    met = [where(z, at_y(k), t) for k in (1, 2, 3)] + [where(z, y, at_t(k)) for k in range(1, T)]
    if SPLIT_GREETING:
        met += [where(at_z(k), y, t) for k in (1, 2, -1, -2)]
    else:
        met += [where(at_z(k), y, t) for k in range(1, Z)]
        met += [where(at_z(k), at_y(j), t) for k in (1, 2, -1, -2) for j in (1, 2, 3)]
    for device in met:
        pl.semaphore_signal(barrier, inc=1, device_id=device, device_id_type=MESH)

    loads = [
        (x_h, x), (bq_h, bases.at[:, 0:128]), (bv_h, bases.at[:, 128:256]),
        (cq_h, cq.at[:, 0:128]), (cq_h, cq.at[:, 128:256]),
        (cv_h, cv.at[0:128]), (cv_h, cv.at[128:256]),
        (wq_h, wq), (wv_h, wv),
        (fq_h, olds_q.at[0]), (sq_h, olds_q.at[1]), (fv_h, olds_v.at[0]), (sv_h, olds_v.at[1]),
    ]
    local = [pltpu.make_async_copy(src, dst, lsem.at[n]) for n, (src, dst) in enumerate(loads)]
    for copy in local:
        copy.start()

    for copy in local[7:]:
        copy.wait()
    gathered[0, 4, 0:16] = wv[...]
    gathered[0, 4, 16:24] = jnp.concatenate([wq[0:8], wq[8:16]], axis=1)
    old[b, 0] = olds_v[0]
    old[b, 1] = olds_v[1]
    old[b, 2] = jnp.concatenate([olds_q[0], olds_q[0]], axis=1)
    old[b, 3] = jnp.concatenate([olds_q[1], olds_q[1]], axis=1)

    pending = []

    def send(copy):
        copy.start()
        pending.append(copy)
        return copy

    pl.semaphore_wait(barrier, len(met))

    def near_copy(n):
        k = NEAR[n]
        return remote(gathered.at[0, 4], gathered.at[0, 4 - k], nsend.at[n], nrecv.at[n], where(at_z(k), y, t))

    if SPLIT_GREETING:
        for k in (2, -2):
            pl.semaphore_signal(greet.at[0], inc=1, device_id=where(at_z(k), y, t), device_id_type=MESH)
    for n in range(4):
        send(near_copy(n))

    for copy in local[0:7]:
        copy.wait()
    reduced = nn(x[...], bases[...])
    high, low = two_parts(reduced)
    both = jnp.concatenate([high, low], axis=0)
    p, r = iota((128, 128), 0), iota((128, 128), 1)
    hlq = nt(one_hot(rank_of(query_order, p) == r), both[:, 0:128]).astype(BF16)
    hlv = nt(one_hot(rank_of(value_order, p) == r), both[:, 128:256]).astype(BF16)
    part_q = nt(hlq, cq[...])
    part_v = nn(hlv, cv[...])
    part_q = jnp.concatenate([part_q[0:64], part_q[64:128]], axis=1)
    for j in range(Y):
        part[j, 0:32] = part_v[32 * j : 32 * j + 32]
        part[j, 32:48] = part_q[16 * j : 16 * j + 16]

    def y_copy(k):
        return remote(part.at[at_y(k)], from_y.at[Y - 1 - k], ysend.at[k - 1], yrecv.at[Y - 1 - k], where(z, at_y(k), t))

    for k in (2, 1, 3):
        send(y_copy(k))

    if SPLIT_GREETING:
        pl.semaphore_wait(greet.at[0], 2)
        for k in (4, -4):
            pl.semaphore_signal(greet.at[1], inc=1, device_id=where(at_z(k), y, t), device_id_type=MESH)
    for n in range(4, 8):
        send(near_copy(n))
    if SPLIT_GREETING:
        pl.semaphore_wait(greet.at[1], 2)

    def old_copy(n):
        k = (4, 8, 12)[n]
        return remote(old.at[b], old.at[b], osend.at[n], orecv.at[n], where(at_z(k), y, t))

    for n in range(3):
        send(old_copy(n))

    for k in (1, 2, 3):
        remote(part.at[0], from_y.at[k - 1], ysend.at[k - 1], yrecv.at[k - 1], where(z, y, t)).wait_recv()
    summed = part[y] + from_y[0] + from_y[1] + from_y[2]
    for j in range(4):
        chunk[j, 0] = summed[8 * j : 8 * j + 4]
        chunk[j, 1] = summed[8 * j + 4 : 8 * j + 8]
        chunk[j, 2] = summed[32 + 4 * j : 36 + 4 * j]
    from_z[z] = chunk[a]

    def z_copy(k):
        there = at_z(k)
        return remote(chunk.at[lax.rem(there, 4)], from_z.at[z], zsend.at[k], zrecv.at[k], where(there, y, t))

    for k in FAR:
        send(z_copy(k))

    for n, k in enumerate(NEAR):
        remote(gathered.at[0, 4], gathered.at[0, 4 - k], nsend.at[n], nrecv.at[n], where(z, y, t)).wait_recv()
    relays = [(k, 0) for k in (4, 3, 2, 1)] + [(-k, 8) for k in (3, 2, 1)]
    for n, (k, slot) in enumerate(relays):
        send(remote(gathered.at[0, slot], gathered.at[0, (slot - k) % 16], rsend.at[n], rrecv.at[n], where(at_z(k), y, t)))

    def w_copy(k, piece):
        rows = pl.ds(0, 9) if piece == 0 else pl.ds(9, 7)
        n = 3 * piece + k - 1
        return remote(
            gathered.at[0, rows], gathered.at[Y - k, rows], wsend.at[n], wrecv.at[n], where(z, at_y(k), t)
        )

    for k in (2, 1, 3):
        send(w_copy(k, 0))

    r, p = iota((128, 256), 0), iota((128, 256), 1) & 127
    bq2[...] = nn(bases[:, 0:128], one_hot(rank_of(query_order, p) == r)).astype(BF16)
    bv2[...] = nn(bases[:, 128:256], one_hot(rank_of(value_order, p) == r)).astype(BF16)

    for n in range(3):
        remote(old.at[0], old.at[0], osend.at[n], orecv.at[n], where(z, y, t)).wait_recv()
    left = iota((2, 128), 1) < 64
    for j in range(4):
        h, i = j // 2, 2 * (j % 2)
        mine = left if h == 0 else jnp.logical_not(left)
        old_first[h, i : i + 2] = old[j, 0]
        old_second[h, i : i + 2] = old[j, 1]
        if h == 0:
            old_first[2, i : i + 2] = old[j, 2]
            old_second[2, i : i + 2] = old[j, 3]
        else:
            old_first[2, i : i + 2] = jnp.where(mine, old[j, 2], old_first[2, i : i + 2])
            old_second[2, i : i + 2] = jnp.where(mine, old[j, 3], old_second[2, i : i + 2])

    for k in range(1, Z):
        remote(chunk.at[0], from_z.at[0], zsend.at[k], zrecv.at[k], where(z, y, t)).wait_recv()
    projected = from_z[0]
    for j in range(1, Z):
        projected = projected + from_z[j]
    first_new = 0.9 * old_first[...] + 0.1 * projected
    second_new = 0.99 * old_second[...] + 0.01 * projected * projected
    direction = first_new / (jnp.sqrt(second_new) + 1e-08)
    send_ag[...] = direction
    mom_o[0] = first_new
    mom_o[1] = second_new
    c = 4 * y + a
    from_ag[c] = direction

    targets = [(k, j) for k in (2, 1, -1, 0) for j in (2, 1, 3, 0) if (k, j) != (0, 0)]
    for n, (k, j) in enumerate(targets):
        send(remote(send_ag, from_ag.at[c], asend.at[n], arecv.at[n], where(at_z(k), at_y(j), t)))

    for n, (k, slot) in enumerate(relays):
        remote(gathered.at[0, 0], gathered.at[0, (slot - k) % 16], rsend.at[n], rrecv.at[n], where(z, y, t)).wait_recv()
    for k in (2, 1, 3):
        send(w_copy(k, 1))

    for n in range(len(targets)):
        remote(send_ag, from_ag.at[0], asend.at[n], arecv.at[n], where(z, y, t)).wait_recv()

    square_q, square_v = None, None
    for j in range(16):
        now = from_ag[j]
        q_now = now[2] * now[2]
        v_now = now[0] * now[0] + now[1] * now[1]
        square_q = q_now if square_q is None else square_q + q_now
        square_v = v_now if square_v is None else square_v + v_now
        dv[8 * j : 8 * j + 4] = now[0]
        dv[8 * j + 4 : 8 * j + 8] = now[1]
        dqp[4 * j : 4 * j + 4] = now[2]
    squares[0] = square_q
    squares[1] = square_v
    tp_o[t, 0] = square_q
    tp_o[t, 1] = square_v
    for k in (4, 3, 5, 2, 6, 1, 7):
        send(remote(squares, tp_o.at[t], tsend.at[k], trecv.at[k], where(z, y, at_t(k))))

    vh, vl = two_parts(dv[...])
    uv_o[...] = nn(bv2[...], jnp.concatenate([vh, vl], axis=0))
    turned = jnp.transpose(dqp[...])
    qt = jnp.concatenate([turned[0:64], turned[64:128]], axis=1)
    qh, ql = two_parts(qt)
    qt2 = jnp.concatenate([qh, ql], axis=1)
    uqt_o[...] = nt(qt2, bq2[...])
    own = pl.multiple_of((z * Y + y) * ROWS, ROWS)
    uq_o[...] = nt(bq2[pl.ds(own, ROWS)], qt2)

    for n in range(6):
        piece, k = n // 3, n % 3 + 1
        rows = pl.ds(0, 9) if piece == 0 else pl.ds(9, 7)
        remote(
            gathered.at[0, rows], gathered.at[Y - k, rows], wsend.at[n], wrecv.at[n], where(z, y, t)
        ).wait_recv()

    def place(n, carry):
        slot, dy = lax.div(n, 4), lax.rem(n, 4)
        row = (lax.rem(z + slot + 12, Z) * Y + lax.rem(y + dy, Y)) * ROWS
        row = pl.multiple_of(row, ROWS)
        wv_o[pl.ds(row, 16)] = gathered[dy, slot, 0:16]
        packed = gathered[dy, slot, 16:24]
        wqn[pl.ds(row, 8)] = packed
        wqn[pl.ds(pl.multiple_of(row + 8, 8), 8)] = pltpu.roll(packed, 64, 1)
        return carry

    lax.fori_loop(0, 64, place, 0)
    for j in range(8):
        wqt_o[:, 128 * j : 128 * j + 128] = jnp.transpose(wqn[128 * j : 128 * j + 128])[0:64]

    for k in range(1, T):
        remote(squares, tp_o.at[0], tsend.at[k], trecv.at[k], where(z, y, t)).wait_recv()
    for copy in pending:
        copy.wait_send()


def finish(
    uv, uqt, uq, wv, wqt, mom, tp, wq_own, wv_own,
    uq_o, uv_o, wq_o, wv_o, fq_o, sq_o, fv_o, sv_o, cq_o, cv_o,
):
    z, y = lax.axis_index("fs"), lax.axis_index("rep")
    b = lax.div(z, 4)
    total = tp[0]
    for k in range(1, T):
        total = total + tp[k]
    sum_q = jnp.sum(jnp.sum(total[0], axis=1, keepdims=True), axis=0, keepdims=True)
    sum_v = jnp.sum(jnp.sum(total[1], axis=1, keepdims=True), axis=0, keepdims=True)
    scale_q = 1.0 / jnp.sqrt(sum_q / (RANK * QL * T) + 1.0)
    scale_v = 1.0 / jnp.sqrt(sum_v / (RANK * VL * T) + 1.0)

    cv_o[...] = (wv[...] - 0.01 * (uv[...] * scale_v)).astype(BF16)
    cq_o[...] = (wqt[...] - 0.01 * (uqt[...] * scale_q)).astype(BF16)
    own = pl.multiple_of((z * Y + y) * ROWS, ROWS)
    update_q = uq[...] * scale_q
    update_v = uv[pl.ds(own, ROWS)] * scale_v
    uq_o[...] = update_q
    uv_o[...] = update_v
    wq_o[...] = wq_own[...] - 0.01 * update_q
    wv_o[...] = wv_own[...] - 0.01 * update_v

    for n, (q_out, v_out) in enumerate(((fq_o, fv_o), (sq_o, sv_o))):
        q_rows, v_rows = None, None
        for j in range(4):
            h, i = j // 2, 2 * (j % 2)
            v_now = mom[n, h, i : i + 2]
            q_now = mom[n, 2, i : i + 2, 64 * h : 64 * h + 64]
            q_rows = q_now if q_rows is None else jnp.where(b == j, q_now, q_rows)
            v_rows = v_now if v_rows is None else jnp.where(b == j, v_now, v_rows)
        q_out[...] = q_rows
        v_out[...] = v_rows


def body(x, cq, cv, bq, bv, wq, wv, fq, sq, fv, sv):
    anywhere = pl.BlockSpec(memory_space=pl.ANY)
    inside = pl.BlockSpec(memory_space=pltpu.VMEM)
    shape = jax.ShapeDtypeStruct
    dma = pltpu.SemaphoreType.DMA
    middle = pl.pallas_call(
        exchange,
        out_shape=(
            shape((D, VL), F32), shape((QL, D), F32), shape((ROWS, QL), F32),
            shape((D, VL), F32), shape((QL, D), F32),
            shape((2, 3, 4, 128), F32), shape((T, 2, 4, 128), F32),
        ),
        in_specs=[anywhere] * 11,
        out_specs=[inside] * 7,
        scratch_shapes=[
            pltpu.VMEM((128, D), BF16), pltpu.VMEM((QL, 256), BF16), pltpu.VMEM((256, VL), BF16),
            pltpu.VMEM((D, 256), BF16), pltpu.VMEM((ROWS, QL), F32), pltpu.VMEM((ROWS, VL), F32),
            pltpu.VMEM((2, 2, QL), F32), pltpu.VMEM((2, 2, VL), F32),
            pltpu.VMEM((Y, Z, 24, 128), F32), pltpu.VMEM((4, 4, 2, 128), F32),
            pltpu.VMEM((Y, 48, 128), F32), pltpu.VMEM((Y - 1, 48, 128), F32),
            pltpu.VMEM((4, 3, 4, 128), F32), pltpu.VMEM((Z, 3, 4, 128), F32),
            pltpu.VMEM((3, 4, 128), F32), pltpu.VMEM((3, 4, 128), F32),
            pltpu.VMEM((3, 4, 128), F32), pltpu.VMEM((16, 3, 4, 128), F32),
            pltpu.VMEM((D, 256), BF16), pltpu.VMEM((D, 256), BF16),
            pltpu.VMEM((128, 128), F32), pltpu.VMEM((64, 128), F32),
            pltpu.VMEM((D, 128), F32), pltpu.VMEM((2, 4, 128), F32),
            dma((13,)), dma((3,)), dma((3,)), dma((Z,)), dma((Z,)), dma((8,)), dma((8,)),
            dma((7,)), dma((7,)), dma((6,)), dma((6,)), dma((3,)), dma((3,)),
            dma((15,)), dma((15,)), dma((T,)), dma((T,)),
            pltpu.SemaphoreType.REGULAR((2,)),
        ],
        compiler_params=pltpu.CompilerParams(collective_id=0, has_side_effects=True),
        name="exchange",
    )(x, cq.T, cv, bq, bv, wq, wv, fq, sq, fv, sv)
    outs = pl.pallas_call(
        finish,
        out_shape=(
            shape((ROWS, QL), F32), shape((ROWS, VL), F32), shape((ROWS, QL), F32), shape((ROWS, VL), F32),
            shape((2, QL), F32), shape((2, QL), F32), shape((2, VL), F32), shape((2, VL), F32),
            shape((QL, D), BF16), shape((D, VL), BF16),
        ),
        in_specs=[inside] * 9,
        out_specs=[inside] * 10,
        name="finish",
    )(*middle, wq, wv)
    return (*outs[:8], outs[8].T, outs[9])


def solution(mesh):
    rows = P(("fs", "rep"), "tp")
    in_specs = (P(("fs", "rep"), None), rows, rows, P(), P()) + (rows,) * 6
    out_specs = (rows,) * 8 + (P(None, "tp"),) * 2
    return jax.shard_map(body, mesh=mesh, in_specs=in_specs, out_specs=out_specs, check_vma=False)
```

```python
import functools

import jax
import jax.numpy as jnp
from jax import lax
from jax.experimental import pallas as pl
from jax.experimental.pallas import tpu as pltpu
from jax.sharding import PartitionSpec as P

F32 = jnp.float32
BF16 = jnp.bfloat16
MESH = pl.DeviceIdType.MESH

Z, Y, T = 16, 4, 8
D, RANK = 1024, 128
QL, VL = 64, 128
ROWS = 16

ROUNDS = ((-2, -1, 0, 1, 2), (-4, -3, 3, 4), (-6, -5, 5, 6), (-7, 7, 8))
SLOT = {rel: n for n, rel in enumerate(sum(ROUNDS, ()))}
STARTS = (0, 5, 9, 13)

PART, CHUNK, DIRECTION, SQUARES, OLD, OLDER, ROUND, WEIGHTS, KINDS = 0, 1, 2, 3, 4, 5, 6, 10, 14


def query_order(p):
    return p >> 6, (p >> 2) & 15, p & 3


def value_order(p):
    return (p >> 2) & 1, p >> 3, p & 3


def rank_of(order, p):
    h, c, i = order(p)
    return 32 * (2 * h + (i >> 1)) + 8 * (c & 3) + 2 * (c >> 2) + (i & 1)


def iota(shape, dim):
    return lax.broadcasted_iota(jnp.int32, shape, dim)


def one_hot(match):
    return jnp.where(match, 1.0, 0.0).astype(F32).astype(BF16)


def nt(a, b):
    return lax.dot_general(a, b, (((1,), (1,)), ((), ())), preferred_element_type=F32)


def nn(a, b):
    return jnp.dot(a, b, preferred_element_type=F32)


def two_parts(value):
    high = value.astype(BF16)
    return high, (value - high.astype(F32)).astype(BF16)


def exchange(
    x_h, cq_h, cv_h, bq_h, bv_h, wq_h, wv_h, fq_h, sq_h, fv_h, sv_h,
    uv_o, uq_o, wv_o, wq_o, mom_o, tp_o,
    x, cq, cv, bases, wq, wv, olds_q, olds_v,
    gathered, old, part, from_y, chunk, from_z, old_first, old_second, send_ag, from_ag,
    bq2, bv2, dv, dqp, squares,
    lsem, sends, recvs, greet,
):
    z, y, t = lax.axis_index("fs"), lax.axis_index("rep"), lax.axis_index("tp")
    a = lax.rem(z, 4)
    b = lax.div(z, 4)

    def at_z(k):
        return lax.rem(z + (k % Z), Z)

    def at_y(k):
        return lax.rem(y + (k % Y), Y)

    def at_t(k):
        return lax.rem(t + (k % T), T)

    def where(zz, yy, tt):
        return (zz, yy, tt)

    def remote(src, dst, kind, device):
        return pltpu.make_async_remote_copy(
            src_ref=src, dst_ref=dst, send_sem=sends.at[kind], recv_sem=recvs.at[kind], device_id=device, device_id_type=MESH
        )

    def arrived(kind, whole):
        remote(whole, whole, kind, where(z, y, t)).wait_recv()

    def left(kind, whole):
        remote(whole, whole, kind, where(z, y, t)).wait_send()

    barrier = pltpu.get_barrier_semaphore()
    met = [where(z, at_y(k), t) for k in (1, 2, 3)] + [where(z, y, at_t(k)) for k in range(1, T)]
    met += [where(at_z(k), y, t) for k in (1, 2, -1, -2)]
    for device in met:
        pl.semaphore_signal(barrier, inc=1, device_id=device, device_id_type=MESH)

    loads = [
        (x_h, x), (bq_h, bases.at[:, 0:128]), (bv_h, bases.at[:, 128:256]),
        (cq_h, cq.at[:, 0:128]), (cq_h, cq.at[:, 128:256]),
        (cv_h, cv.at[0:128]), (cv_h, cv.at[128:256]),
        (wq_h, wq), (wv_h, wv),
        (fq_h, olds_q.at[0]), (sq_h, olds_q.at[1]), (fv_h, olds_v.at[0]), (sv_h, olds_v.at[1]),
    ]
    groups = (0, 1, 1, 2, 2, 3, 3, 4, 5, 6, 6, 7, 7)
    local = [pltpu.make_async_copy(src, dst, lsem.at[groups[n]]) for n, (src, dst) in enumerate(loads)]
    for copy in local:
        copy.start()

    def loaded(group, whole):
        pltpu.make_async_copy(whole, whole, lsem.at[group]).wait()

    loaded(0, x)
    loaded(1, bases)
    reduced = nn(x[...], bases[...])
    high, low = two_parts(reduced)
    both = jnp.concatenate([high, low], axis=0)

    for group, whole in ((2, cq), (3, cv), (4, wq), (5, wv), (6, olds_q), (7, olds_v)):
        loaded(group, whole)
    gathered[0, SLOT[0], 0:16] = wv[...]
    gathered[0, SLOT[0], 16:24] = jnp.concatenate([wq[0:8], wq[8:16]], axis=1)
    old[b, 0] = olds_v[0]
    old[b, 1] = olds_v[1]
    old[b, 2] = jnp.concatenate([olds_q[0], olds_q[1]], axis=1)

    pl.semaphore_wait(barrier, len(met))
    for k in (2, -2):
        pl.semaphore_signal(greet.at[0], inc=1, device_id=where(at_z(k), y, t), device_id_type=MESH)

    def round_copies(level):
        if level == 0:
            moves = [(0, k) for k in (2, -2, 1, -1)]
        else:
            moves = [(-2 * level, 2), (2 * level, -2), (-2 * level, 1), (2 * level, -1)]
        copies = []
        for n, (rel, k) in enumerate(moves):
            there = rel - k
            if there == 8 and k < 0:
                continue
            there = 8 if there == -8 else there
            copies.append(remote(gathered.at[0, SLOT[rel]], gathered.at[0, SLOT[there]], ROUND + level, where(at_z(k), y, t)))
        return copies

    def level_rows(level):
        return pl.ds(STARTS[level], len(ROUNDS[level]))

    def w_copy(k, level):
        rows = level_rows(level)
        return remote(gathered.at[0, rows], gathered.at[Y - k, rows], WEIGHTS + level, where(z, at_y(k), t))

    def go_on(level):
        arrived(ROUND + level, gathered.at[0, pl.ds(0, 3 if level == 3 else 4)])
        if level < 3:
            for copy in round_copies(level + 1):
                copy.start()
        for k in (2, 1, 3):
            w_copy(k, level).start()

    for copy in round_copies(0):
        copy.start()

    p, r = iota((128, 128), 0), iota((128, 128), 1)
    hlq = nt(one_hot(rank_of(query_order, p) == r), both[:, 0:128]).astype(BF16)
    hlv = nt(one_hot(rank_of(value_order, p) == r), both[:, 128:256]).astype(BF16)
    part_q = nt(hlq, cq[...])
    part_v = nn(hlv, cv[...])
    part_q = jnp.concatenate([part_q[0:64], part_q[64:128]], axis=1)
    for j in range(Y):
        part[j, 0:32] = part_v[32 * j : 32 * j + 32]
        part[j, 32:48] = part_q[16 * j : 16 * j + 16]

    def y_copy(k):
        return remote(part.at[at_y(k)], from_y.at[Y - 1 - k], PART, where(z, at_y(k), t))

    for k in (2, 1, 3):
        y_copy(k).start()

    pl.semaphore_wait(greet.at[0], 2)
    for k in (4, -4):
        pl.semaphore_signal(greet.at[1], inc=1, device_id=where(at_z(k), y, t), device_id_type=MESH)

    for k in (4, -4):
        remote(old.at[b], old.at[b], OLD, where(at_z(k), y, t)).start()

    go_on(0)

    arrived(PART, from_y)
    summed = part[y] + from_y[0] + from_y[1] + from_y[2]
    for j in range(4):
        chunk[j, 0] = summed[8 * j : 8 * j + 4]
        chunk[j, 1] = summed[8 * j + 4 : 8 * j + 8]
        chunk[j, 2] = summed[32 + 4 * j : 36 + 4 * j]
    from_z[z] = chunk[a]

    def z_copy(k):
        there = at_z(k)
        return remote(chunk.at[lax.rem(there, 4)], from_z.at[z], CHUNK, where(there, y, t))

    for k in (4, 12, 3, 13, 2, 14, 1, 15):
        z_copy(k).start()

    pl.semaphore_wait(greet.at[1], 2)
    for k in (8, 7, 9, 6, 10, 5, 11):
        z_copy(k).start()

    go_on(1)
    arrived(OLD, old.at[pl.ds(0, 2)])
    before = lax.rem(b + 3, 4)
    remote(old.at[before], old.at[before], OLDER, where(at_z(4), y, t)).start()

    r, p = iota((128, 256), 0), iota((128, 256), 1) & 127
    bq2[...] = nn(bases[:, 0:128], one_hot(rank_of(query_order, p) == r)).astype(BF16)
    bv2[...] = nn(bases[:, 128:256], one_hot(rank_of(value_order, p) == r)).astype(BF16)

    go_on(2)

    arrived(OLDER, old.at[0])
    lower = iota((2, 128), 1) < 64
    for i in (0, 2):
        low_half, high_half = old[i // 2, 2], old[i // 2 + 2, 2]
        for h in range(2):
            old_first[h, i : i + 2] = old[i // 2 + 2 * h, 0]
            old_second[h, i : i + 2] = old[i // 2 + 2 * h, 1]
        old_first[2, i : i + 2] = jnp.where(lower, low_half, pltpu.roll(high_half, 64, 1))
        old_second[2, i : i + 2] = jnp.where(lower, pltpu.roll(low_half, 64, 1), high_half)

    arrived(CHUNK, from_z.at[pl.ds(0, 15)])
    projected = from_z[0]
    for j in range(1, Z):
        projected = projected + from_z[j]
    first_new = 0.9 * old_first[...] + 0.1 * projected
    second_new = 0.99 * old_second[...] + 0.01 * projected * projected
    direction = first_new / (jnp.sqrt(second_new) + 1e-08)
    send_ag[...] = direction
    mom_o[0] = first_new
    mom_o[1] = second_new
    c = 4 * y + a
    from_ag[c] = direction

    targets = [(k, j) for k in (2, 1, -1, 0) for j in (2, 1, 3, 0) if (k, j) != (0, 0)]
    for k, j in targets:
        remote(send_ag, from_ag.at[c], DIRECTION, where(at_z(k), at_y(j), t)).start()

    go_on(3)

    def place(level):
        arrived(WEIGHTS + level, gathered.at[pl.ds(1, 3), level_rows(level)])
        for rel in ROUNDS[level]:
            for dy in range(Y):
                row = (at_z(rel) * Y + at_y(dy)) * ROWS
                row = pl.multiple_of(row, ROWS)
                wv_o[pl.ds(row, 16)] = gathered[dy, SLOT[rel], 0:16]
                packed = gathered[dy, SLOT[rel], 16:24]
                wq_o[pl.ds(row, 8)] = packed
                wq_o[pl.ds(pl.multiple_of(row + 8, 8), 8)] = pltpu.roll(packed, 64, 1)

    place(0)
    place(1)

    arrived(DIRECTION, from_ag.at[pl.ds(0, 15)])

    square_q, square_v = None, None
    for j in range(16):
        now = from_ag[j]
        q_now = now[2] * now[2]
        v_now = now[0] * now[0] + now[1] * now[1]
        square_q = q_now if square_q is None else square_q + q_now
        square_v = v_now if square_v is None else square_v + v_now
        dv[8 * j : 8 * j + 4] = now[0]
        dv[8 * j + 4 : 8 * j + 8] = now[1]
        dqp[4 * j : 4 * j + 4] = now[2]
    squares[0] = square_q
    squares[1] = square_v
    tp_o[t, 0] = square_q
    tp_o[t, 1] = square_v
    for k in (4, 3, 5, 2, 6, 1, 7):
        remote(squares, tp_o.at[t], SQUARES, where(z, y, at_t(k))).start()

    vh, vl = two_parts(dv[...])
    uv_o[...] = nn(bv2[...], jnp.concatenate([vh, vl], axis=0))
    qh, ql = two_parts(jnp.concatenate([dqp[:, 0:64], dqp[:, 64:128]], axis=0))
    uq_o[...] = nn(bq2[...], jnp.concatenate([qh, ql], axis=0))

    place(2)
    place(3)

    arrived(SQUARES, tp_o.at[pl.ds(0, 7)])

    left(PART, from_y)
    left(CHUNK, from_z.at[pl.ds(0, 15)])
    left(DIRECTION, from_ag.at[pl.ds(0, 15)])
    left(SQUARES, tp_o.at[pl.ds(0, 7)])
    left(OLD, old.at[pl.ds(0, 2)])
    left(OLDER, old.at[0])
    for level in range(4):
        left(ROUND + level, gathered.at[0, pl.ds(0, 3 if level == 3 else 4)])
        left(WEIGHTS + level, gathered.at[pl.ds(1, 3), level_rows(level)])


def finish(
    uv, uq, wv, wq, mom, tp,
    uq_o, uv_o, wq_o, wv_o, fq_o, sq_o, fv_o, sv_o, cq_o, cv_o,
):
    z, y = lax.axis_index("fs"), lax.axis_index("rep")
    b = lax.div(z, 4)
    total = tp[0]
    for k in range(1, T):
        total = total + tp[k]
    sum_q = jnp.sum(jnp.sum(total[0], axis=1, keepdims=True), axis=0, keepdims=True)
    sum_v = jnp.sum(jnp.sum(total[1], axis=1, keepdims=True), axis=0, keepdims=True)
    scale_q = 1.0 / jnp.sqrt(sum_q / (RANK * QL * T) + 1.0)
    scale_v = 1.0 / jnp.sqrt(sum_v / (RANK * VL * T) + 1.0)

    half_q = (wq[:, 0:64] - 0.01 * (uq[...] * scale_q)).astype(BF16)
    same = one_hot(iota((QL, QL), 0) == iota((QL, QL), 1))
    cq_o[...] = nt(same, half_q).astype(BF16)
    cv_o[...] = (wv[...] - 0.01 * (uv[...] * scale_v)).astype(BF16)
    own = pl.multiple_of((z * Y + y) * ROWS, ROWS)
    update_q = uq[pl.ds(own, ROWS)] * scale_q
    update_v = uv[pl.ds(own, ROWS)] * scale_v
    uq_o[...] = update_q
    uv_o[...] = update_v
    wq_o[...] = wq[pl.ds(own, ROWS), 0:64] - 0.01 * update_q
    wv_o[...] = wv[pl.ds(own, ROWS)] - 0.01 * update_v

    for n, (q_out, v_out) in enumerate(((fq_o, fv_o), (sq_o, sv_o))):
        q_rows, v_rows = None, None
        for j in range(4):
            h, i = j // 2, 2 * (j % 2)
            v_now = mom[n, h, i : i + 2]
            q_now = mom[n, 2, i : i + 2, 64 * h : 64 * h + 64]
            q_rows = q_now if q_rows is None else jnp.where(b == j, q_now, q_rows)
            v_rows = v_now if v_rows is None else jnp.where(b == j, v_now, v_rows)
        q_out[...] = q_rows
        v_out[...] = v_rows


def body(x, cq, cv, bq, bv, wq, wv, fq, sq, fv, sv):
    anywhere = pl.BlockSpec(memory_space=pltpu.HBM)
    inside = pl.BlockSpec(memory_space=pltpu.VMEM)
    shape = jax.ShapeDtypeStruct
    dma = pltpu.SemaphoreType.DMA
    middle = pl.pallas_call(
        exchange,
        out_shape=(
            shape((D, VL), F32), shape((D, QL), F32), shape((D, VL), F32), shape((D, 128), F32),
            shape((2, 3, 4, 128), F32), shape((T, 2, 4, 128), F32),
        ),
        in_specs=[anywhere] * 11,
        out_specs=[inside] * 6,
        scratch_shapes=[
            pltpu.VMEM((128, D), BF16), pltpu.VMEM((QL, 256), BF16), pltpu.VMEM((256, VL), BF16),
            pltpu.VMEM((D, 256), BF16), pltpu.VMEM((ROWS, QL), F32), pltpu.VMEM((ROWS, VL), F32),
            pltpu.VMEM((2, 2, QL), F32), pltpu.VMEM((2, 2, VL), F32),
            pltpu.VMEM((Y, Z, 24, 128), F32), pltpu.VMEM((4, 3, 2, 128), F32),
            pltpu.VMEM((Y, 48, 128), F32), pltpu.VMEM((Y - 1, 48, 128), F32),
            pltpu.VMEM((4, 3, 4, 128), F32), pltpu.VMEM((Z, 3, 4, 128), F32),
            pltpu.VMEM((3, 4, 128), F32), pltpu.VMEM((3, 4, 128), F32),
            pltpu.VMEM((3, 4, 128), F32), pltpu.VMEM((16, 3, 4, 128), F32),
            pltpu.VMEM((D, 256), BF16), pltpu.VMEM((D, 256), BF16),
            pltpu.VMEM((128, 128), F32), pltpu.VMEM((64, 128), F32),
            pltpu.VMEM((2, 4, 128), F32),
            dma((8,)), dma((KINDS,)), dma((KINDS,)),
            pltpu.SemaphoreType.REGULAR((2,)),
        ],
        compiler_params=pltpu.CompilerParams(collective_id=0, has_side_effects=True, vmem_limit_bytes=12 << 20),
        name="exchange",
    )(*(pltpu.with_memory_space_constraint(a, pltpu.HBM) for a in (x, cq.T, cv, bq, bv, wq, wv, fq, sq, fv, sv)))
    outs = pl.pallas_call(
        finish,
        out_shape=(
            shape((ROWS, QL), F32), shape((ROWS, VL), F32), shape((ROWS, QL), F32), shape((ROWS, VL), F32),
            shape((2, QL), F32), shape((2, QL), F32), shape((2, VL), F32), shape((2, VL), F32),
            shape((QL, D), BF16), shape((D, VL), BF16),
        ),
        in_specs=[inside] * 6,
        out_specs=[inside] * 10,
        compiler_params=pltpu.CompilerParams(vmem_limit_bytes=12 << 20),
        name="finish",
    )(*middle)
    return (*outs[:8], outs[8].T, outs[9])


def solution(mesh):
    rows = P(("fs", "rep"), "tp")
    in_specs = (P(("fs", "rep"), None), rows, rows, P(), P()) + (rows,) * 6
    out_specs = (rows,) * 8 + (P(None, "tp"),) * 2
    return jax.shard_map(body, mesh=mesh, in_specs=in_specs, out_specs=out_specs, check_vma=False)
```

```python
import functools

import jax
import jax.numpy as jnp
from jax import lax
from jax.experimental import pallas as pl
from jax.experimental.pallas import tpu as pltpu
from jax.sharding import PartitionSpec as P

F32 = jnp.float32
BF16 = jnp.bfloat16
MESH = pl.DeviceIdType.MESH

Z, Y, T, X = 16, 4, 8, 4
D, RANK = 1024, 128
QL, VL = 64, 128
ROWS = 16

ROUNDS = ((-3, -2, -1, 0, 1, 2, 3), (-6, -5, -4, 4, 5, 6), (-7, 7, 8))
SLOT = {rel: n for n, rel in enumerate(sum(ROUNDS, ()))}
STARTS = (0, 7, 13)
MOVES = (
    ((0, 3, -3), (0, -3, 3), (0, 2, -2), (0, -2, 2), (0, 1, -1), (0, -1, 1)),
    ((-3, 3, -6), (3, -3, 6), (-3, 2, -5), (3, -2, 5), (-3, 1, -4), (3, -1, 4)),
    ((-6, 2, 8), (-6, 1, -7), (6, -1, 7)),
)

PART, CHUNK, DIRECTION, DIRECTION_0, SQUARES, MOMENTS, OWN_OLD, OLD, OLDER = range(9)
ROUND, WEIGHTS, KINDS = 9, 12, 15


def query_order(p):
    return p >> 6, (p >> 2) & 15, p & 3


def value_order(p):
    return (p >> 2) & 1, p >> 3, p & 3


def rank_of(order, p):
    h, c, i = order(p)
    a = 2 * (c & 1) + ((c >> 1) & 1)
    return 32 * (2 * h + (i >> 1)) + 8 * a + 2 * (c >> 2) + (i & 1)


def iota(shape, dim):
    return lax.broadcasted_iota(jnp.int32, shape, dim)


def one_hot(match):
    return jnp.where(match, 1.0, 0.0).astype(F32).astype(BF16)


def nt(a, b):
    return lax.dot_general(a, b, (((1,), (1,)), ((), ())), preferred_element_type=F32)


def nn(a, b):
    return jnp.dot(a, b, preferred_element_type=F32)


def two_parts(value):
    high = value.astype(BF16)
    return high, (value - high.astype(F32)).astype(BF16)


def exchange(
    x_h, cq_h, cv_h, bq_h, bv_h, wq_h, wv_h, fq_h, sq_h, fv_h, sv_h,
    uv_o, uq_o, wv_o, wq_o, mom_o, squares_o,
    x, cq, cv, bases, wq, wv, olds_q, olds_v,
    gathered, own_old, old, part, from_y, chunk, from_z, old_first, old_second, send_ag, from_ag,
    bq2, bv2, dv, dqp, square, room,
    lsem, sends, recvs, greet,
):
    z, y, t = lax.axis_index("fs"), lax.axis_index("rep"), lax.axis_index("tp")
    a = lax.rem(z, 4)
    b = lax.div(z, 4)
    xi = lax.div(t, 2)
    core = lax.rem(t, 2)
    t0, t1 = 2 * xi, 2 * xi + 1
    c = 4 * y + 2 * lax.rem(a, 2) + lax.div(a, 2)
    odd = lax.rem(z, 2)
    pair, mate = lax.div(z, 2), z + 1 - 2 * odd

    def at_z(k):
        return lax.rem(z + (k % Z), Z)

    def at_y(k):
        return lax.rem(y + (k % Y), Y)

    def at_x(k, core_there):
        return 2 * lax.rem(xi + (k % X), X) + core_there

    def remote(src, dst, kind, device):
        return pltpu.make_async_remote_copy(
            src_ref=src, dst_ref=dst, send_sem=sends.at[kind], recv_sem=recvs.at[kind], device_id=device, device_id_type=MESH
        )

    def arrived(kind, whole):
        remote(whole, whole, kind, (z, y, t)).wait_recv()

    def left(kind, whole):
        remote(whole, whole, kind, (z, y, t)).wait_send()

    def hello(semaphore, device):
        pl.semaphore_signal(semaphore, inc=1, device_id=device, device_id_type=MESH)

    barrier = pltpu.get_barrier_semaphore()
    for k in range(Y):
        @pl.when(core == 1)
        def _():
            hello(barrier, (z, at_y(k), t0))
            hello(barrier, (mate, at_y(k), t0))
            if k:
                hello(barrier, (z, at_y(k), t1))
                hello(barrier, (mate, at_y(k), t1))

        @pl.when(core == 0)
        def _():
            hello(barrier, (z, at_y(k), t1))

            if k:
                hello(barrier, (z, at_y(k), t0))

    for k in (3, -3, 2, -2, 1, -1):
        hello(barrier, (at_z(k), y, t))
    for k in range(1, X):
        hello(barrier, (z, y, at_x(k, 1)))

    loads = [
        (x_h, x), (bq_h, bases.at[:, 0:128]), (bv_h, bases.at[:, 128:256]),
        (cq_h, cq.at[:, 0:128]), (cq_h, cq.at[:, 128:256]),
        (cv_h, cv.at[0:128]), (cv_h, cv.at[128:256]),
        (wq_h, wq), (wv_h, wv),
        (fq_h, olds_q.at[0]), (sq_h, olds_q.at[1]), (fv_h, olds_v.at[0]), (sv_h, olds_v.at[1]),
    ]
    groups = (0, 1, 1, 2, 2, 3, 3, 4, 5, 6, 6, 7, 7)
    for n, (src, dst) in enumerate(loads):
        pltpu.make_async_copy(src, dst, lsem.at[groups[n]]).start()

    def loaded(group, whole):
        pltpu.make_async_copy(whole, whole, lsem.at[group]).wait()

    loaded(0, x)
    loaded(1, bases)
    reduced = nn(x[...], bases[...])
    high, low = two_parts(reduced)
    both = jnp.concatenate([high, low], axis=0)

    for group, whole in ((2, cq), (3, cv), (4, wq), (5, wv), (6, olds_q), (7, olds_v)):
        loaded(group, whole)
    gathered[0, SLOT[0], 0:16] = wv[...]
    gathered[0, SLOT[0], 16:24] = jnp.concatenate([wq[0:8], wq[8:16]], axis=1)
    own_old[0] = olds_v[0]
    own_old[1] = olds_v[1]
    own_old[2] = jnp.concatenate([olds_q[0], olds_q[1]], axis=1)

    def round_copies(level):
        for rel, k, there in MOVES[level]:
            remote(gathered.at[0, SLOT[rel]], gathered.at[0, SLOT[there]], ROUND + level, (at_z(k), y, t)).start()

    def level_rows(level):
        return pl.ds(STARTS[level], len(ROUNDS[level]))

    def round_wait_shape(level):
        return gathered.at[0, pl.ds(0, len(MOVES[level]))]

    def go_on(level):
        arrived(ROUND + level, round_wait_shape(level))
        if level < 2:
            round_copies(level + 1)
        rows = level_rows(level)
        for k in (2, 1, 3):
            remote(gathered.at[0, rows], gathered.at[Y - k, rows], WEIGHTS + level, (z, at_y(k), t)).start()

    p, r = iota((128, 128), 0), iota((128, 128), 1)
    hlq = nt(one_hot(rank_of(query_order, p) == r), both[:, 0:128]).astype(BF16)
    hlv = nt(one_hot(rank_of(value_order, p) == r), both[:, 128:256]).astype(BF16)
    part_q = nt(hlq, cq[...])
    part_v = nn(hlv, cv[...])
    part_q = jnp.concatenate([part_q[0:64], part_q[64:128]], axis=1)
    for j in range(Y):
        for n in range(2):
            m = 2 * j + n
            part[j, n, 0:16] = part_v[16 * m : 16 * m + 16]
            part[j, n, 16:24] = part_q[8 * m : 8 * m + 8]

    @pl.when(core == 1)
    def _():
        pl.semaphore_wait(barrier, 22)
        for k in (3, -3):
            hello(greet.at[0], (at_z(k), y, t))

    @pl.when(core == 0)
    def _():
        pl.semaphore_wait(barrier, 17)
        remote(own_old, old.at[b, 0], OWN_OLD, (z, y, t1)).start()

    def part_copy(n, k):
        slot = 2 * (Y * n + (Y - k) % Y) + core
        there, parity = (mate, 1 - odd) if n else (z, odd)
        remote(part.at[at_y(k), parity], from_y.at[slot], PART, (there, at_y(k), t1)).start()

    for k in (2, 1, 3, 0):
        for n in (1, 0):
            if n or k:
                part_copy(n, k)

    @pl.when(core == 0)
    def _():
        part_copy(0, 0)

    round_copies(0)

    def permuted_bases():
        r, p = iota((128, 256), 0), iota((128, 256), 1) & 127
        bq2[...] = nn(bases[:, 0:128], one_hot(rank_of(query_order, p) == r)).astype(BF16)
        bv2[...] = nn(bases[:, 128:256], one_hot(rank_of(value_order, p) == r)).astype(BF16)

    def place(level):
        arrived(WEIGHTS + level, gathered.at[pl.ds(1, 3), level_rows(level)])
        for rel in ROUNDS[level]:
            for dy in range(Y):
                row = (at_z(rel) * Y + at_y(dy)) * ROWS
                row = pl.multiple_of(row, ROWS)
                wv_o[pl.ds(row, 16)] = gathered[dy, SLOT[rel], 0:16]
                packed = gathered[dy, SLOT[rel], 16:24]
                wq_o[pl.ds(row, 8)] = packed
                wq_o[pl.ds(pl.multiple_of(row + 8, 8), 8)] = pltpu.roll(packed, 64, 1)

    def weights_left():
        for level in range(3):
            left(ROUND + level, round_wait_shape(level))
            left(WEIGHTS + level, gathered.at[pl.ds(1, 3), level_rows(level)])

    def updates():
        for j in range(16):
            dv[8 * j : 8 * j + 4] = from_ag[j, 0]
            dv[8 * j + 4 : 8 * j + 8] = from_ag[j, 1]
            dqp[4 * j : 4 * j + 4] = from_ag[j, 2]
        vh, vl = two_parts(dv[...])
        uv_o[...] = nn(bv2[...], jnp.concatenate([vh, vl], axis=0))
        qh, ql = two_parts(jnp.concatenate([dqp[:, 0:64], dqp[:, 64:128]], axis=0))
        uq_o[...] = nn(bq2[...], jnp.concatenate([qh, ql], axis=0))

    @pl.when(core == 0)
    def _():
        permuted_bases()
        go_on(0)
        go_on(1)
        place(0)
        go_on(2)
        place(1)
        arrived(DIRECTION_0, from_ag)
        updates()
        place(2)
        arrived(SQUARES, squares_o)
        arrived(MOMENTS, mom_o)
        left(OWN_OLD, own_old)
        left(PART, from_y.at[pl.ds(0, 8)])
        weights_left()

    @pl.when(core == 1)
    def _():
        old[b, 1] = own_old[...]
        arrived(OWN_OLD, own_old)
        pl.semaphore_wait(greet.at[0], 2)
        for k in (2, -2):
            hello(greet.at[1], (at_z(k), y, t))
        for k in (4, -4):
            remote(old.at[b], old.at[b], OLD, (at_z(k), y, t)).start()
        arrived(PART, from_y.at[pl.ds(0, 15)])
        summed = [from_y[0], part[y, odd]]
        for j in range(1, 2 * Y):
            summed = [summed[0] + from_y[2 * j], summed[1] + from_y[2 * j + 1]]
        for j in range(2):
            for n, now in enumerate(summed):
                chunk[j, 3 * n] = now[8 * j : 8 * j + 4]
                chunk[j, 3 * n + 1] = now[8 * j + 4 : 8 * j + 8]
                chunk[j, 3 * n + 2] = now[16 + 4 * j : 20 + 4 * j]
        from_z[pair] = chunk[lax.rem(pair, 2)]

        def z_copy(k):
            there = at_z(k)
            remote(chunk.at[lax.rem(lax.div(there, 2), 2)], from_z.at[pair], CHUNK, (there, y, t)).start()

        for k in (6, 10):
            z_copy(k)

        pl.semaphore_wait(greet.at[1], 2)
        for k in (8, 4, 12, 2, 14):
            z_copy(k)


        go_on(0)

        arrived(OLD, old.at[pl.ds(0, 2)])
        before = lax.rem(b + 3, 4)
        remote(old.at[before], old.at[before], OLDER, (at_z(4), y, t)).start()

        go_on(1)

        permuted_bases()

        arrived(OLDER, old.at[0])
        lower = iota((2, 128), 1) < 64
        for n in range(2):
            for i in (0, 2):
                low_half, high_half = old[i // 2, n, 2], old[i // 2 + 2, n, 2]
                for h in range(2):
                    old_first[3 * n + h, i : i + 2] = old[i // 2 + 2 * h, n, 0]
                    old_second[3 * n + h, i : i + 2] = old[i // 2 + 2 * h, n, 1]
                old_first[3 * n + 2, i : i + 2] = jnp.where(lower, low_half, pltpu.roll(high_half, 64, 1))
                old_second[3 * n + 2, i : i + 2] = jnp.where(lower, pltpu.roll(low_half, 64, 1), high_half)

        arrived(CHUNK, from_z.at[pl.ds(0, 7)])
        projected = from_z[0]
        for j in range(1, Z // 2):
            projected = projected + from_z[j]
        first_new = 0.9 * old_first[...] + 0.1 * projected
        second_new = 0.99 * old_second[...] + 0.01 * projected * projected
        direction = first_new / (jnp.sqrt(second_new) + 1e-08)
        send_ag[0] = direction
        squared = direction * direction
        square_q = squared[2] + squared[5]
        square_v = squared[0] + squared[1] + squared[3] + squared[4]
        square_q = jnp.sum(square_q, axis=0, keepdims=True)
        square_v = jnp.sum(square_v, axis=0, keepdims=True)
        square_q = square_q + pltpu.roll(square_q, 64, 1)
        square_v = square_v + pltpu.roll(square_v, 64, 1)
        row = jnp.where(iota((1, 128), 1) < 64, square_q, square_v)
        square[...] = row
        there = 16 * xi + c
        def send_squares(dxs):
            for dx in dxs:
                for k in (2, 1, -1, 0):
                    for j in (2, 1, 3, 0):
                        for n in range(2):
                            if (dx, k, j, n) != (0, 0, 0, 1):
                                remote(square, squares_o.at[there], SQUARES, (at_z(k), at_y(j), at_x(dx, n))).start()

        send_squares((2, 1, 3))
        for k in (2, 1, -1, 0):
            for j in (2, 1, 3, 0):
                remote(send_ag.at[0, pl.ds(0, 3)], from_ag.at[c], DIRECTION_0, (at_z(k), at_y(j), t0)).start()
                if (k, j) != (0, 0):
                    remote(send_ag.at[0, pl.ds(3, 3)], from_ag.at[c], DIRECTION, (at_z(k), at_y(j), t)).start()
        send_squares((0,))
        squares_o[there] = row
        from_ag[c] = direction[3:6]
        send_ag[1] = first_new
        send_ag[2] = second_new
        mom_o[0] = first_new[3:6]
        mom_o[1] = second_new[3:6]
        remote(send_ag.at[pl.ds(1, 2), pl.ds(0, 3)], mom_o, MOMENTS, (z, y, t0)).start()

        go_on(2)

        place(0)
        place(1)

        arrived(DIRECTION, from_ag.at[pl.ds(0, 15)])
        updates()
        place(2)

        arrived(SQUARES, squares_o.at[pl.ds(0, 63)])

        left(PART, from_y.at[pl.ds(0, 7)])
        left(CHUNK, from_z.at[pl.ds(0, 7)])
        left(DIRECTION, from_ag.at[pl.ds(0, 15)])
        left(DIRECTION_0, from_ag)
        left(MOMENTS, mom_o)
        left(OLD, old.at[pl.ds(0, 2)])
        left(OLDER, old.at[0])
        weights_left()
        left(SQUARES, room)


def finish(
    uv, uq, wv, wq, mom, squares,
    uq_o, uv_o, wq_o, wv_o, fq_o, sq_o, fv_o, sv_o, cq_o, cv_o,
):
    z, y = lax.axis_index("fs"), lax.axis_index("rep")
    b = lax.div(z, 4)
    total = squares[0]
    for k in range(1, 16 * X):
        total = total + squares[k]
    query_lanes = iota((1, 128), 1) < 64
    sum_q = jnp.sum(jnp.where(query_lanes, total, 0.0), axis=1, keepdims=True)
    sum_v = jnp.sum(jnp.where(query_lanes, 0.0, total), axis=1, keepdims=True)
    scale_q = 1.0 / jnp.sqrt(sum_q / (RANK * QL * T) + 1.0)
    scale_v = 1.0 / jnp.sqrt(sum_v / (RANK * VL * T) + 1.0)

    half_q = (wq[:, 0:64] - 0.01 * (uq[...] * scale_q)).astype(BF16)
    same = one_hot(iota((QL, QL), 0) == iota((QL, QL), 1))
    cq_o[...] = nt(same, half_q).astype(BF16)
    cv_o[...] = (wv[...] - 0.01 * (uv[...] * scale_v)).astype(BF16)
    own = pl.multiple_of((z * Y + y) * ROWS, ROWS)
    update_q = uq[pl.ds(own, ROWS)] * scale_q
    update_v = uv[pl.ds(own, ROWS)] * scale_v
    uq_o[...] = update_q
    uv_o[...] = update_v
    wq_o[...] = wq[pl.ds(own, ROWS), 0:64] - 0.01 * update_q
    wv_o[...] = wv[pl.ds(own, ROWS)] - 0.01 * update_v

    for n, (q_out, v_out) in enumerate(((fq_o, fv_o), (sq_o, sv_o))):
        q_rows, v_rows = None, None
        for j in range(4):
            h, i = j // 2, 2 * (j % 2)
            v_now = mom[n, h, i : i + 2]
            q_now = mom[n, 2, i : i + 2, 64 * h : 64 * h + 64]
            q_rows = q_now if q_rows is None else jnp.where(b == j, q_now, q_rows)
            v_rows = v_now if v_rows is None else jnp.where(b == j, v_now, v_rows)
        q_out[...] = q_rows
        v_out[...] = v_rows


def body(x, cq, cv, bq, bv, wq, wv, fq, sq, fv, sv):
    anywhere = pl.BlockSpec(memory_space=pltpu.HBM)
    inside = pl.BlockSpec(memory_space=pltpu.VMEM)
    shape = jax.ShapeDtypeStruct
    dma = pltpu.SemaphoreType.DMA
    middle = pl.pallas_call(
        exchange,
        out_shape=(
            shape((D, VL), F32), shape((D, QL), F32), shape((D, VL), F32), shape((D, 128), F32),
            shape((2, 3, 4, 128), F32), shape((16 * X, 1, 128), F32),
        ),
        in_specs=[anywhere] * 11,
        out_specs=[inside] * 6,
        scratch_shapes=[
            pltpu.VMEM((128, D), BF16), pltpu.VMEM((QL, 256), BF16), pltpu.VMEM((256, VL), BF16),
            pltpu.VMEM((D, 256), BF16), pltpu.VMEM((ROWS, QL), F32), pltpu.VMEM((ROWS, VL), F32),
            pltpu.VMEM((2, 2, QL), F32), pltpu.VMEM((2, 2, VL), F32),
            pltpu.VMEM((Y, Z, 24, 128), F32),
            pltpu.VMEM((3, 2, 128), F32), pltpu.VMEM((4, 2, 3, 2, 128), F32),
            pltpu.VMEM((Y, 2, 24, 128), F32), pltpu.VMEM((4 * Y, 24, 128), F32),
            pltpu.VMEM((2, 6, 4, 128), F32), pltpu.VMEM((Z // 2, 6, 4, 128), F32),
            pltpu.VMEM((6, 4, 128), F32), pltpu.VMEM((6, 4, 128), F32),
            pltpu.VMEM((3, 6, 4, 128), F32), pltpu.VMEM((16, 3, 4, 128), F32),
            pltpu.VMEM((D, 256), BF16), pltpu.VMEM((D, 256), BF16),
            pltpu.VMEM((128, 128), F32), pltpu.VMEM((64, 128), F32), pltpu.VMEM((1, 128), F32),
            pltpu.VMEM((127, 1, 128), F32),
            dma((8,)), dma((KINDS,)), dma((KINDS,)),
            pltpu.SemaphoreType.REGULAR((2,)),
        ],
        compiler_params=pltpu.CompilerParams(collective_id=0, has_side_effects=True, vmem_limit_bytes=12 << 20),
        name="exchange",
    )(*(pltpu.with_memory_space_constraint(a, pltpu.HBM) for a in (x, cq.T, cv, bq, bv, wq, wv, fq, sq, fv, sv)))
    outs = pl.pallas_call(
        finish,
        out_shape=(
            shape((ROWS, QL), F32), shape((ROWS, VL), F32), shape((ROWS, QL), F32), shape((ROWS, VL), F32),
            shape((2, QL), F32), shape((2, QL), F32), shape((2, VL), F32), shape((2, VL), F32),
            shape((QL, D), BF16), shape((D, VL), BF16),
        ),
        in_specs=[inside] * 6,
        out_specs=[inside] * 10,
        compiler_params=pltpu.CompilerParams(vmem_limit_bytes=12 << 20),
        name="finish",
    )(*middle)
    return (*outs[:8], outs[8].T, outs[9])


def solution(mesh):
    rows = P(("fs", "rep"), "tp")
    in_specs = (P(("fs", "rep"), None), rows, rows, P(), P()) + (rows,) * 6
    out_specs = (rows,) * 8 + (P(None, "tp"),) * 2
    return jax.shard_map(body, mesh=mesh, in_specs=in_specs, out_specs=out_specs, check_vma=False)
```

```python
import jax
import jax.numpy as jnp
from jax import lax
from jax.experimental import pallas as pl
from jax.experimental.pallas import tpu as pltpu
from jax.sharding import PartitionSpec as P

F32 = jnp.float32
BF16 = jnp.bfloat16
MESH = pl.DeviceIdType.MESH

Z, Y, T, X = 16, 4, 8, 4
D, RANK = 1024, 128
QL, VL = 64, 128
ROWS = 16

ROUNDS = ((-3, -2, -1, 0, 1, 2, 3), (-6, -5, -4, 4, 5, 6), (-7, 7, 8))
SLOT = {rel: n for n, rel in enumerate(sum(ROUNDS, ()))}
STARTS = (0, 7, 13)
MOVES = (
    ((0, 3, -3), (0, -3, 3), (0, 2, -2), (0, -2, 2), (0, 1, -1), (0, -1, 1)),
    ((-3, 3, -6), (3, -3, 6), (-3, 2, -5), (3, -2, 5), (-3, 1, -4), (3, -1, 4)),
    ((-6, 2, 8), (-6, 1, -7), (6, -1, 7)),
)

PART, CHUNK, DIRECTION, DIRECTION_0, SQUARES, MOMENTS, OWN_OLD, OLD = range(8)
ROUND, WEIGHTS, KINDS = 8, 11, 14


def query_order(p):
    return p >> 6, (p >> 2) & 15, p & 3


def value_order(p):
    return (p >> 2) & 1, p >> 3, p & 3


def rank_of(order, p):
    h, c, i = order(p)
    a = 2 * (c & 1) + ((c >> 1) & 1)
    return 32 * (2 * h + (i >> 1)) + 8 * a + 2 * (c >> 2) + (i & 1)


def iota(shape, dim):
    return lax.broadcasted_iota(jnp.int32, shape, dim)


def one_hot(match):
    return jnp.where(match, 1.0, 0.0).astype(F32).astype(BF16)


def nt(a, b):
    return lax.dot_general(a, b, (((1,), (1,)), ((), ())), preferred_element_type=F32)


def nn(a, b):
    return jnp.dot(a, b, preferred_element_type=F32)


def two_parts(value):
    high = value.astype(BF16)
    return high, (value - high.astype(F32)).astype(BF16)


def exchange(
    x_h, cq_h, cv_h, bq_h, bv_h, wq_h, wv_h, fq_h, sq_h, fv_h, sv_h,
    uv_o, uq_o, wv_o, wq_o, mom_o, squares_o,
    x, cq, cv, bases, wq, wv, olds_q, olds_v,
    gathered, own_old, old, part, from_y, chunk, from_z, old_first, old_second, send_ag, from_ag,
    bq2, bv2, dv, dqp, square, room,
    lsem, sends, recvs, greet,
):
    z, y, t = lax.axis_index("fs"), lax.axis_index("rep"), lax.axis_index("tp")
    a = lax.rem(z, 4)
    b = lax.div(z, 4)
    xi = lax.div(t, 2)
    core = lax.rem(t, 2)
    t0, t1 = 2 * xi, 2 * xi + 1
    c = 4 * y + 2 * lax.rem(a, 2) + lax.div(a, 2)
    odd = lax.rem(z, 2)
    pair, mate = lax.div(z, 2), z + 1 - 2 * odd

    def at_z(k):
        return lax.rem(z + (k % Z), Z)

    def at_y(k):
        return lax.rem(y + (k % Y), Y)

    def at_x(k, core_there):
        return 2 * lax.rem(xi + (k % X), X) + core_there

    def remote(src, dst, kind, device):
        return pltpu.make_async_remote_copy(
            src_ref=src, dst_ref=dst, send_sem=sends.at[kind], recv_sem=recvs.at[kind], device_id=device, device_id_type=MESH
        )

    def arrived(kind, whole):
        remote(whole, whole, kind, (z, y, t)).wait_recv()

    def left(kind, whole):
        remote(whole, whole, kind, (z, y, t)).wait_send()

    def hello(semaphore, device):
        pl.semaphore_signal(semaphore, inc=1, device_id=device, device_id_type=MESH)

    barrier = pltpu.get_barrier_semaphore()
    for k in range(Y):
        @pl.when(core == 1)
        def _():
            hello(barrier, (z, at_y(k), t0))
            hello(barrier, (mate, at_y(k), t0))
            if k:
                hello(barrier, (z, at_y(k), t1))
                hello(barrier, (mate, at_y(k), t1))

        @pl.when(core == 0)
        def _():
            hello(barrier, (z, at_y(k), t1))

            if k:
                hello(barrier, (z, at_y(k), t0))

    for k in (3, -3, 2, -2, 1, -1):
        hello(barrier, (at_z(k), y, t))
    for k in range(1, X):
        hello(barrier, (z, y, at_x(k, 1)))

    loads = [
        (x_h, x), (bq_h, bases.at[:, 0:128]), (bv_h, bases.at[:, 128:256]),
        (cq_h, cq.at[:, 0:128]), (cq_h, cq.at[:, 128:256]),
        (cv_h, cv.at[0:128]), (cv_h, cv.at[128:256]),
        (wq_h, wq), (wv_h, wv),
        (fq_h, olds_q.at[0]), (sq_h, olds_q.at[1]), (fv_h, olds_v.at[0]), (sv_h, olds_v.at[1]),
    ]
    groups = (0, 1, 1, 2, 2, 3, 3, 4, 5, 6, 6, 7, 7)
    for n, (src, dst) in enumerate(loads):
        pltpu.make_async_copy(src, dst, lsem.at[groups[n]]).start()

    def loaded(group, whole):
        pltpu.make_async_copy(whole, whole, lsem.at[group]).wait()

    loaded(0, x)
    loaded(1, bases)
    reduced = nn(x[...], bases[...])
    high, low = two_parts(reduced)
    both = jnp.concatenate([high, low], axis=0)

    for group, whole in ((2, cq), (3, cv), (4, wq), (5, wv), (6, olds_q), (7, olds_v)):
        loaded(group, whole)
    gathered[0, SLOT[0], 0:16] = wv[...]
    gathered[0, SLOT[0], 16:24] = jnp.concatenate([wq[0:8], wq[8:16]], axis=1)
    own_old[0] = olds_v[0]
    own_old[1] = olds_v[1]
    own_old[2] = jnp.concatenate([olds_q[0], olds_q[1]], axis=1)

    def round_copies(level):
        for rel, k, there in MOVES[level]:
            remote(gathered.at[0, SLOT[rel]], gathered.at[0, SLOT[there]], ROUND + level, (at_z(k), y, t)).start()

    def level_rows(level):
        return pl.ds(STARTS[level], len(ROUNDS[level]))

    def round_wait_shape(level):
        return gathered.at[0, pl.ds(0, len(MOVES[level]))]

    def go_on(level):
        arrived(ROUND + level, round_wait_shape(level))
        rows = level_rows(level)
        if level == 0:
            round_copies(1)
        for k in (2, 1, 3):
            remote(gathered.at[0, rows], gathered.at[Y - k, rows], WEIGHTS + level, (z, at_y(k), t)).start()
        if level == 1:
            round_copies(2)

    p, r = iota((128, 128), 0), iota((128, 128), 1)
    hlq = nt(one_hot(rank_of(query_order, p) == r), both[:, 0:128]).astype(BF16)
    hlv = nt(one_hot(rank_of(value_order, p) == r), both[:, 128:256]).astype(BF16)
    part_q = nt(hlq, cq[...])
    part_v = nn(hlv, cv[...])
    part_q = jnp.concatenate([part_q[0:64], part_q[64:128]], axis=1)
    for j in range(Y):
        for n in range(2):
            m = 2 * j + n
            part[j, n, 0:16] = part_v[16 * m : 16 * m + 16]
            part[j, n, 16:24] = part_q[8 * m : 8 * m + 8]

    @pl.when(core == 1)
    def _():
        pl.semaphore_wait(barrier, 22)
        for k in (3, -3):
            hello(greet.at[0], (at_z(k), y, t))

    @pl.when(core == 0)
    def _():
        pl.semaphore_wait(barrier, 17)
        remote(own_old, old.at[b, 0], OWN_OLD, (z, y, t1)).start()

    def part_copy(n, k):
        slot = 2 * (Y * n + (Y - k) % Y) + core
        there, parity = (mate, 1 - odd) if n else (z, odd)
        remote(part.at[at_y(k), parity], from_y.at[slot], PART, (there, at_y(k), t1)).start()

    for k in (2, 1, 3, 0):
        for n in (1, 0):
            if n or k:
                part_copy(n, k)

    @pl.when(core == 0)
    def _():
        part_copy(0, 0)

    round_copies(0)

    def permuted_bases():
        r, p = iota((128, 256), 0), iota((128, 256), 1) & 127
        bq2[...] = nn(bases[:, 0:128], one_hot(rank_of(query_order, p) == r)).astype(BF16)
        bv2[...] = nn(bases[:, 128:256], one_hot(rank_of(value_order, p) == r)).astype(BF16)

    def place(level):
        arrived(WEIGHTS + level, gathered.at[pl.ds(1, 3), level_rows(level)])
        for rel in ROUNDS[level]:
            for dy in range(Y):
                row = (at_z(rel) * Y + at_y(dy)) * ROWS
                row = pl.multiple_of(row, ROWS)
                wv_o[pl.ds(row, 16)] = gathered[dy, SLOT[rel], 0:16]
                packed = gathered[dy, SLOT[rel], 16:24]
                wq_o[pl.ds(row, 8)] = packed
                wq_o[pl.ds(pl.multiple_of(row + 8, 8), 8)] = pltpu.roll(packed, 64, 1)

    def weights_left():
        for level in range(3):
            left(ROUND + level, round_wait_shape(level))
            left(WEIGHTS + level, gathered.at[pl.ds(1, 3), level_rows(level)])

    def updates():
        for j in range(16):
            dv[8 * j : 8 * j + 4] = from_ag[j, 0]
            dv[8 * j + 4 : 8 * j + 8] = from_ag[j, 1]
            dqp[4 * j : 4 * j + 4] = from_ag[j, 2]
        vh, vl = two_parts(dv[...])
        uv_o[...] = nn(bv2[...], jnp.concatenate([vh, vl], axis=0))
        qh, ql = two_parts(jnp.concatenate([dqp[:, 0:64], dqp[:, 64:128]], axis=0))
        uq_o[...] = nn(bq2[...], jnp.concatenate([qh, ql], axis=0))

    @pl.when(core == 0)
    def _():
        permuted_bases()
        go_on(0)
        go_on(1)
        place(0)
        go_on(2)
        place(1)
        arrived(DIRECTION_0, from_ag)
        updates()
        place(2)
        arrived(SQUARES, squares_o)
        arrived(MOMENTS, mom_o)
        left(OWN_OLD, own_old)
        left(PART, from_y.at[pl.ds(0, 8)])
        weights_left()

    @pl.when(core == 1)
    def _():
        old[b, 1] = own_old[...]
        arrived(OWN_OLD, own_old)
        pl.semaphore_wait(greet.at[0], 2)
        for k in (2, -2):
            hello(greet.at[1], (at_z(k), y, t))
        for k in (4, -4):
            remote(old.at[b], old.at[b], OLD, (at_z(k), y, t)).start()
        arrived(ROUND, round_wait_shape(0))
        round_copies(1)

        arrived(PART, from_y.at[pl.ds(0, 15)])
        summed = [from_y[0], part[y, odd]]
        for j in range(1, 2 * Y):
            summed = [summed[0] + from_y[2 * j], summed[1] + from_y[2 * j + 1]]
        for j in range(2):
            for n, now in enumerate(summed):
                chunk[j, 3 * n] = now[8 * j : 8 * j + 4]
                chunk[j, 3 * n + 1] = now[8 * j + 4 : 8 * j + 8]
                chunk[j, 3 * n + 2] = now[16 + 4 * j : 20 + 4 * j]
        from_z[pair] = chunk[lax.rem(pair, 2)]

        def z_copy(k):
            there = at_z(k)
            remote(chunk.at[lax.rem(lax.div(there, 2), 2)], from_z.at[pair], CHUNK, (there, y, t)).start()

        for k in (6, 10):
            z_copy(k)

        pl.semaphore_wait(greet.at[1], 2)
        z_copy(8)
        remote(old.at[b], old.at[b], OLD, (at_z(8), y, t)).start()
        for k in (4, 12, 2, 14):
            z_copy(k)


        for k in (2, 1, 3):
            remote(
                gathered.at[0, level_rows(0)], gathered.at[Y - k, level_rows(0)], WEIGHTS, (z, at_y(k), t)
            ).start()

        go_on(1)

        permuted_bases()

        arrived(OLD, old.at[pl.ds(0, 3)])
        lower = iota((2, 128), 1) < 64
        for n in range(2):
            for i in (0, 2):
                low_half, high_half = old[i // 2, n, 2], old[i // 2 + 2, n, 2]
                for h in range(2):
                    old_first[3 * n + h, i : i + 2] = old[i // 2 + 2 * h, n, 0]
                    old_second[3 * n + h, i : i + 2] = old[i // 2 + 2 * h, n, 1]
                old_first[3 * n + 2, i : i + 2] = jnp.where(lower, low_half, pltpu.roll(high_half, 64, 1))
                old_second[3 * n + 2, i : i + 2] = jnp.where(lower, pltpu.roll(low_half, 64, 1), high_half)

        arrived(CHUNK, from_z.at[pl.ds(0, 7)])
        projected = from_z[0]
        for j in range(1, Z // 2):
            projected = projected + from_z[j]
        first_new = 0.9 * old_first[...] + 0.1 * projected
        second_new = 0.99 * old_second[...] + 0.01 * projected * projected
        direction = first_new / (jnp.sqrt(second_new) + 1e-08)
        send_ag[0] = direction
        squared = direction * direction
        square_q = squared[2] + squared[5]
        square_v = squared[0] + squared[1] + squared[3] + squared[4]
        square_q = jnp.sum(square_q, axis=0, keepdims=True)
        square_v = jnp.sum(square_v, axis=0, keepdims=True)
        square_q = square_q + pltpu.roll(square_q, 64, 1)
        square_v = square_v + pltpu.roll(square_v, 64, 1)
        row = jnp.where(iota((1, 128), 1) < 64, square_q, square_v)
        square[...] = row
        there = 16 * xi + c
        def send_squares(dxs):
            for dx in dxs:
                for k in (-2, 1, -1, 0):
                    for j in (2, 1, 3, 0):
                        for n in range(2):
                            if (dx, k, j, n) != (0, 0, 0, 1):
                                remote(square, squares_o.at[there], SQUARES, (at_z(k), at_y(j), at_x(dx, n))).start()

        send_squares((2, 1, 3))
        for k in (-2, 1, -1, 0):
            for j in (2, 1, 3, 0):
                remote(send_ag.at[0, pl.ds(0, 3)], from_ag.at[c], DIRECTION_0, (at_z(k), at_y(j), t0)).start()
                if (k, j) != (0, 0):
                    remote(send_ag.at[0, pl.ds(3, 3)], from_ag.at[c], DIRECTION, (at_z(k), at_y(j), t)).start()
        send_squares((0,))
        squares_o[there] = row
        from_ag[c] = direction[3:6]
        send_ag[1] = first_new
        send_ag[2] = second_new
        mom_o[0] = first_new[3:6]
        mom_o[1] = second_new[3:6]
        remote(send_ag.at[pl.ds(1, 2), pl.ds(0, 3)], mom_o, MOMENTS, (z, y, t0)).start()

        go_on(2)

        place(0)
        place(1)

        arrived(DIRECTION, from_ag.at[pl.ds(0, 15)])
        updates()
        place(2)

        arrived(SQUARES, squares_o.at[pl.ds(0, 63)])

        left(PART, from_y.at[pl.ds(0, 7)])
        left(CHUNK, from_z.at[pl.ds(0, 7)])
        left(DIRECTION, from_ag.at[pl.ds(0, 15)])
        left(DIRECTION_0, from_ag)
        left(MOMENTS, mom_o)
        left(OLD, old.at[pl.ds(0, 3)])
        weights_left()
        left(SQUARES, room)


def finish(
    uv, uq, wv, wq, mom, squares,
    uq_o, uv_o, wq_o, wv_o, fq_o, sq_o, fv_o, sv_o, cq_o, cv_o,
):
    z, y = lax.axis_index("fs"), lax.axis_index("rep")
    b = lax.div(z, 4)
    sums = [squares[k] for k in range(16 * X)]
    while len(sums) > 1:
        sums = [sums[k] + sums[k + 1] for k in range(0, len(sums), 2)]
    total = sums[0]
    query_lanes = iota((1, 128), 1) < 64
    sum_q = jnp.sum(jnp.where(query_lanes, total, 0.0), axis=1, keepdims=True)
    sum_v = jnp.sum(jnp.where(query_lanes, 0.0, total), axis=1, keepdims=True)
    scale_q = 1.0 / jnp.sqrt(sum_q / (RANK * QL * T) + 1.0)
    scale_v = 1.0 / jnp.sqrt(sum_v / (RANK * VL * T) + 1.0)

    half_q = (wq[:, 0:64] - 0.01 * (uq[...] * scale_q)).astype(BF16)
    same = one_hot(iota((QL, QL), 0) == iota((QL, QL), 1))
    cq_o[...] = nt(same, half_q).astype(BF16)
    cv_o[...] = (wv[...] - 0.01 * (uv[...] * scale_v)).astype(BF16)
    own = pl.multiple_of((z * Y + y) * ROWS, ROWS)
    update_q = uq[pl.ds(own, ROWS)] * scale_q
    update_v = uv[pl.ds(own, ROWS)] * scale_v
    uq_o[...] = update_q
    uv_o[...] = update_v
    wq_o[...] = wq[pl.ds(own, ROWS), 0:64] - 0.01 * update_q
    wv_o[...] = wv[pl.ds(own, ROWS)] - 0.01 * update_v

    for n, (q_out, v_out) in enumerate(((fq_o, fv_o), (sq_o, sv_o))):
        q_rows, v_rows = None, None
        for j in range(4):
            h, i = j // 2, 2 * (j % 2)
            v_now = mom[n, h, i : i + 2]
            q_now = mom[n, 2, i : i + 2, 64 * h : 64 * h + 64]
            q_rows = q_now if q_rows is None else jnp.where(b == j, q_now, q_rows)
            v_rows = v_now if v_rows is None else jnp.where(b == j, v_now, v_rows)
        q_out[...] = q_rows
        v_out[...] = v_rows


def body(x, cq, cv, bq, bv, wq, wv, fq, sq, fv, sv):
    anywhere = pl.BlockSpec(memory_space=pltpu.HBM)
    inside = pl.BlockSpec(memory_space=pltpu.VMEM)
    shape = jax.ShapeDtypeStruct
    dma = pltpu.SemaphoreType.DMA
    middle = pl.pallas_call(
        exchange,
        out_shape=(
            shape((D, VL), F32), shape((D, QL), F32), shape((D, VL), F32), shape((D, 128), F32),
            shape((2, 3, 4, 128), F32), shape((16 * X, 1, 128), F32),
        ),
        in_specs=[anywhere] * 11,
        out_specs=[inside] * 6,
        scratch_shapes=[
            pltpu.VMEM((128, D), BF16), pltpu.VMEM((QL, 256), BF16), pltpu.VMEM((256, VL), BF16),
            pltpu.VMEM((D, 256), BF16), pltpu.VMEM((ROWS, QL), F32), pltpu.VMEM((ROWS, VL), F32),
            pltpu.VMEM((2, 2, QL), F32), pltpu.VMEM((2, 2, VL), F32),
            pltpu.VMEM((Y, Z, 24, 128), F32),
            pltpu.VMEM((3, 2, 128), F32), pltpu.VMEM((4, 2, 3, 2, 128), F32),
            pltpu.VMEM((Y, 2, 24, 128), F32), pltpu.VMEM((4 * Y, 24, 128), F32),
            pltpu.VMEM((2, 6, 4, 128), F32), pltpu.VMEM((Z // 2, 6, 4, 128), F32),
            pltpu.VMEM((6, 4, 128), F32), pltpu.VMEM((6, 4, 128), F32),
            pltpu.VMEM((3, 6, 4, 128), F32), pltpu.VMEM((16, 3, 4, 128), F32),
            pltpu.VMEM((D, 256), BF16), pltpu.VMEM((D, 256), BF16),
            pltpu.VMEM((128, 128), F32), pltpu.VMEM((64, 128), F32), pltpu.VMEM((1, 128), F32),
            pltpu.VMEM((127, 1, 128), F32),
            dma((8,)), dma((KINDS,)), dma((KINDS,)),
            pltpu.SemaphoreType.REGULAR((2,)),
        ],
        compiler_params=pltpu.CompilerParams(collective_id=0, has_side_effects=True, vmem_limit_bytes=12 << 20),
        name="exchange",
    )(*(pltpu.with_memory_space_constraint(a, pltpu.HBM) for a in (x, cq.T, cv, bq, bv, wq, wv, fq, sq, fv, sv)))
    outs = pl.pallas_call(
        finish,
        out_shape=(
            shape((ROWS, QL), F32), shape((ROWS, VL), F32), shape((ROWS, QL), F32), shape((ROWS, VL), F32),
            shape((2, QL), F32), shape((2, QL), F32), shape((2, VL), F32), shape((2, VL), F32),
            shape((QL, D), BF16), shape((D, VL), BF16),
        ),
        in_specs=[inside] * 6,
        out_specs=[inside] * 10,
        compiler_params=pltpu.CompilerParams(vmem_limit_bytes=12 << 20),
        name="finish",
    )(*middle)
    return (*outs[:8], outs[8].T, outs[9])


def solution(mesh):
    rows = P(("fs", "rep"), "tp")
    in_specs = (P(("fs", "rep"), None), rows, rows, P(), P()) + (rows,) * 6
    out_specs = (rows,) * 8 + (P(None, "tp"),) * 2
    return jax.shard_map(body, mesh=mesh, in_specs=in_specs, out_specs=out_specs, check_vma=False)
```

```python
import jax
import jax.numpy as jnp
from jax import lax
from jax.experimental import pallas as pl
from jax.experimental.pallas import tpu as pltpu
from jax.sharding import PartitionSpec as P

F32 = jnp.float32
BF16 = jnp.bfloat16
MESH = pl.DeviceIdType.MESH

Z, Y, T, X = 16, 4, 8, 4
D, RANK = 1024, 128
QL, VL = 64, 128
ROWS = 16

ROUNDS = ((-3, -2, -1, 0, 1, 2, 3), (-6, -5, -4, 4, 5, 6), (-7, 7, 8))
SLOT = {rel: n for n, rel in enumerate(sum(ROUNDS, ()))}
STARTS = (0, 7, 13)
MOVES = (
    ((0, 3, -3), (0, -3, 3), (0, 2, -2), (0, -2, 2), (0, 1, -1), (0, -1, 1)),
    ((-3, 3, -6), (3, -3, 6), (-3, 2, -5), (3, -2, 5), (-3, 1, -4), (3, -1, 4)),
    ((-6, 2, 8), (-6, 1, -7), (6, -1, 7)),
)

PART, CHUNK, DIRECTION, DIRECTION_0, SQUARES, MOMENTS, OWN_OLD, OLD = range(8)
ROUND, WEIGHTS, KINDS = 8, 11, 14


def query_order(p):
    return p >> 6, (p >> 2) & 15, p & 3


def value_order(p):
    return (p >> 2) & 1, p >> 3, p & 3


def rank_of(order, p):
    h, c, i = order(p)
    a = 2 * (c & 1) + ((c >> 1) & 1)
    return 32 * (2 * h + (i >> 1)) + 8 * a + 2 * (c >> 2) + (i & 1)


def iota(shape, dim):
    return lax.broadcasted_iota(jnp.int32, shape, dim)


def one_hot(match):
    return jnp.where(match, 1.0, 0.0).astype(F32).astype(BF16)


def nt(a, b):
    return lax.dot_general(a, b, (((1,), (1,)), ((), ())), preferred_element_type=F32)


def nn(a, b):
    return jnp.dot(a, b, preferred_element_type=F32)


def two_parts(value):
    high = value.astype(BF16)
    return high, (value - high.astype(F32)).astype(BF16)


def exchange(
    x_h, cq_h, cv_h, bq_h, bv_h, wq_h, wv_h, fq_h, sq_h, fv_h, sv_h,
    uv_o, uq_o, wv_o, wq_o, mom_o, squares_o,
    x, cq, cv, bases, wq, wv, olds_q, olds_v,
    gathered, own_old, old, part, from_y, chunk, from_z, old_first, old_second, send_ag, from_ag,
    bq2, bv2, dv, dqp, square, room,
    lsem, sends, recvs, greet,
):
    z, y, t = lax.axis_index("fs"), lax.axis_index("rep"), lax.axis_index("tp")
    a = lax.rem(z, 4)
    b = lax.div(z, 4)
    xi = lax.div(t, 2)
    core = lax.rem(t, 2)
    t0, t1 = 2 * xi, 2 * xi + 1
    c = 4 * y + 2 * lax.rem(a, 2) + lax.div(a, 2)
    odd = lax.rem(z, 2)
    pair, mate = lax.div(z, 2), z + 1 - 2 * odd

    def at_z(k):
        return lax.rem(z + (k % Z), Z)

    def at_y(k):
        return lax.rem(y + (k % Y), Y)

    def at_x(k, core_there):
        return 2 * lax.rem(xi + (k % X), X) + core_there

    def remote(src, dst, kind, device):
        return pltpu.make_async_remote_copy(
            src_ref=src, dst_ref=dst, send_sem=sends.at[kind], recv_sem=recvs.at[kind], device_id=device, device_id_type=MESH
        )

    def arrived(kind, whole):
        remote(whole, whole, kind, (z, y, t)).wait_recv()

    def left(kind, whole):
        remote(whole, whole, kind, (z, y, t)).wait_send()

    def hello(semaphore, device):
        pl.semaphore_signal(semaphore, inc=1, device_id=device, device_id_type=MESH)

    barrier = pltpu.get_barrier_semaphore()
    for k in (2, 1, 3, 0):
        @pl.when(core == 1)
        def _():
            hello(barrier, (z, at_y(k), t0))
            hello(barrier, (mate, at_y(k), t0))
            if k:
                hello(barrier, (z, at_y(k), t1))
                hello(barrier, (mate, at_y(k), t1))

        @pl.when(core == 0)
        def _():
            hello(barrier, (z, at_y(k), t1))

            if k:
                hello(barrier, (z, at_y(k), t0))

    for k in (3, -3, 2, -2, 1, -1):
        hello(barrier, (at_z(k), y, t))
    for k in range(1, X):
        hello(barrier, (z, y, at_x(k, 1)))

    loads = [
        (x_h, x), (bq_h, bases.at[:, 0:128]), (bv_h, bases.at[:, 128:256]),
        (cq_h, cq.at[:, 0:128]), (cq_h, cq.at[:, 128:256]),
        (cv_h, cv.at[0:128]), (cv_h, cv.at[128:256]),
        (wq_h, wq), (wv_h, wv),
        (fq_h, olds_q.at[0]), (sq_h, olds_q.at[1]), (fv_h, olds_v.at[0]), (sv_h, olds_v.at[1]),
    ]
    groups = (0, 1, 1, 2, 2, 3, 3, 4, 5, 6, 6, 7, 7)
    for n, (src, dst) in enumerate(loads):
        pltpu.make_async_copy(src, dst, lsem.at[groups[n]]).start()

    def loaded(group, whole):
        pltpu.make_async_copy(whole, whole, lsem.at[group]).wait()

    loaded(0, x)
    loaded(1, bases)
    reduced = nn(x[...], bases[...])
    high, low = two_parts(reduced)
    both = jnp.concatenate([high, low], axis=0)

    for group, whole in ((2, cq), (3, cv), (4, wq), (5, wv), (6, olds_q), (7, olds_v)):
        loaded(group, whole)
    gathered[0, SLOT[0], 0:16] = wv[...]
    gathered[0, SLOT[0], 16:24] = jnp.concatenate([wq[0:8], wq[8:16]], axis=1)
    own_old[0] = olds_v[0]
    own_old[1] = olds_v[1]
    own_old[2] = jnp.concatenate([olds_q[0], olds_q[1]], axis=1)

    def round_copies(level):
        for rel, k, there in MOVES[level]:
            remote(gathered.at[0, SLOT[rel]], gathered.at[0, SLOT[there]], ROUND + level, (at_z(k), y, t)).start()

    def level_rows(level):
        return pl.ds(STARTS[level], len(ROUNDS[level]))

    def round_wait_shape(level):
        return gathered.at[0, pl.ds(0, len(MOVES[level]))]

    def go_on(level):
        arrived(ROUND + level, round_wait_shape(level))
        rows = level_rows(level)
        if level == 0:
            round_copies(1)
        for k in (2, 1, 3):
            remote(gathered.at[0, rows], gathered.at[Y - k, rows], WEIGHTS + level, (z, at_y(k), t)).start()
        if level == 1:
            round_copies(2)

    p, r = iota((128, 128), 0), iota((128, 128), 1)
    hlq = nt(one_hot(rank_of(query_order, p) == r), both[:, 0:128]).astype(BF16)
    hlv = nt(one_hot(rank_of(value_order, p) == r), both[:, 128:256]).astype(BF16)
    part_q = nt(hlq, cq[...])
    part_v = nn(hlv, cv[...])
    part_q = jnp.concatenate([part_q[0:64], part_q[64:128]], axis=1)
    for j in range(Y):
        for n in range(2):
            m = 2 * j + n
            part[j, n, 0:16] = part_v[16 * m : 16 * m + 16]
            part[j, n, 16:24] = part_q[8 * m : 8 * m + 8]

    @pl.when(core == 1)
    def _():
        pl.semaphore_wait(barrier, 22)
        for k in (3, -3):
            hello(greet.at[0], (at_z(k), y, t))

    @pl.when(core == 0)
    def _():
        pl.semaphore_wait(barrier, 17)
        remote(own_old, old.at[b, 0], OWN_OLD, (z, y, t1)).start()

    round_copies(0)

    def part_copy(n, k):
        slot = 2 * (Y * n + (Y - k) % Y) + core
        there, parity = (mate, 1 - odd) if n else (z, odd)
        remote(part.at[at_y(k), parity], from_y.at[slot], PART, (there, at_y(k), t1)).start()

    for k in (2, 1, 3, 0):
        for n in (1, 0):
            if n or k:
                part_copy(n, k)

    @pl.when(core == 0)
    def _():
        part_copy(0, 0)

    def permuted_bases():
        r, p = iota((128, 256), 0), iota((128, 256), 1) & 127
        bq2[...] = nn(bases[:, 0:128], one_hot(rank_of(query_order, p) == r)).astype(BF16)
        bv2[...] = nn(bases[:, 128:256], one_hot(rank_of(value_order, p) == r)).astype(BF16)

    def place(level):
        arrived(WEIGHTS + level, gathered.at[pl.ds(1, 3), level_rows(level)])
        for rel in ROUNDS[level]:
            for dy in range(Y):
                row = (at_z(rel) * Y + at_y(dy)) * ROWS
                row = pl.multiple_of(row, ROWS)
                wv_o[pl.ds(row, 16)] = gathered[dy, SLOT[rel], 0:16]
                packed = gathered[dy, SLOT[rel], 16:24]
                wq_o[pl.ds(row, 8)] = packed
                wq_o[pl.ds(pl.multiple_of(row + 8, 8), 8)] = pltpu.roll(packed, 64, 1)

    def weights_left():
        for level in range(3):
            left(ROUND + level, round_wait_shape(level))
            left(WEIGHTS + level, gathered.at[pl.ds(1, 3), level_rows(level)])

    def updates():
        for j in range(16):
            dv[8 * j : 8 * j + 4] = from_ag[j, 0]
            dv[8 * j + 4 : 8 * j + 8] = from_ag[j, 1]
            dqp[4 * j : 4 * j + 4] = from_ag[j, 2]
        vh, vl = two_parts(dv[...])
        uv_o[...] = nn(bv2[...], jnp.concatenate([vh, vl], axis=0))
        qh, ql = two_parts(jnp.concatenate([dqp[:, 0:64], dqp[:, 64:128]], axis=0))
        uq_o[...] = nn(bq2[...], jnp.concatenate([qh, ql], axis=0))

    @pl.when(core == 0)
    def _():
        permuted_bases()
        go_on(0)
        go_on(1)
        place(0)
        go_on(2)
        place(1)
        arrived(DIRECTION_0, from_ag)
        updates()
        place(2)
        arrived(SQUARES, squares_o)
        arrived(MOMENTS, mom_o)
        left(OWN_OLD, own_old)
        left(PART, from_y.at[pl.ds(0, 8)])
        weights_left()

    @pl.when(core == 1)
    def _():
        old[b, 1] = own_old[...]
        arrived(OWN_OLD, own_old)
        pl.semaphore_wait(greet.at[0], 2)
        for k in (2, -2):
            hello(greet.at[1], (at_z(k), y, t))
        for k in (4, -4):
            remote(old.at[b], old.at[b], OLD, (at_z(k), y, t)).start()
        arrived(ROUND, round_wait_shape(0))
        round_copies(1)

        arrived(PART, from_y.at[pl.ds(0, 15)])
        summed = [from_y[0], part[y, odd]]
        for j in range(1, 2 * Y):
            summed = [summed[0] + from_y[2 * j], summed[1] + from_y[2 * j + 1]]
        for j in range(2):
            for n, now in enumerate(summed):
                chunk[j, 3 * n] = now[8 * j : 8 * j + 4]
                chunk[j, 3 * n + 1] = now[8 * j + 4 : 8 * j + 8]
                chunk[j, 3 * n + 2] = now[16 + 4 * j : 20 + 4 * j]
        from_z[pair] = chunk[lax.rem(pair, 2)]

        def z_copy(k):
            there = at_z(k)
            remote(chunk.at[lax.rem(lax.div(there, 2), 2)], from_z.at[pair], CHUNK, (there, y, t)).start()

        for k in (6, 10):
            z_copy(k)

        pl.semaphore_wait(greet.at[1], 2)
        z_copy(8)
        remote(old.at[b], old.at[b], OLD, (at_z(8), y, t)).start()
        for k in (4, 12, 2, 14):
            z_copy(k)


        for k in (2, 1, 3):
            remote(
                gathered.at[0, level_rows(0)], gathered.at[Y - k, level_rows(0)], WEIGHTS, (z, at_y(k), t)
            ).start()

        go_on(1)

        permuted_bases()

        arrived(OLD, old.at[pl.ds(0, 3)])
        lower = iota((2, 128), 1) < 64
        for n in range(2):
            for i in (0, 2):
                low_half, high_half = old[i // 2, n, 2], old[i // 2 + 2, n, 2]
                for h in range(2):
                    old_first[3 * n + h, i : i + 2] = old[i // 2 + 2 * h, n, 0]
                    old_second[3 * n + h, i : i + 2] = old[i // 2 + 2 * h, n, 1]
                old_first[3 * n + 2, i : i + 2] = jnp.where(lower, low_half, pltpu.roll(high_half, 64, 1))
                old_second[3 * n + 2, i : i + 2] = jnp.where(lower, pltpu.roll(low_half, 64, 1), high_half)

        arrived(CHUNK, from_z.at[pl.ds(0, 7)])
        projected = from_z[0]
        for j in range(1, Z // 2):
            projected = projected + from_z[j]
        first_new = 0.9 * old_first[...] + 0.1 * projected
        second_new = 0.99 * old_second[...] + 0.01 * projected * projected
        direction = first_new / (jnp.sqrt(second_new) + 1e-08)
        send_ag[0] = direction
        squared = direction * direction
        square_q = squared[2] + squared[5]
        square_v = squared[0] + squared[1] + squared[3] + squared[4]
        square_q = jnp.sum(square_q, axis=0, keepdims=True)
        square_v = jnp.sum(square_v, axis=0, keepdims=True)
        square_q = square_q + pltpu.roll(square_q, 64, 1)
        square_v = square_v + pltpu.roll(square_v, 64, 1)
        row = jnp.where(iota((1, 128), 1) < 64, square_q, square_v)
        square[...] = row
        there = 16 * xi + c
        def send_squares(k, dxs):
            for dx in dxs:
                for j in (0, 2, 1, 3):
                    for n in range(2):
                        one = remote(square, squares_o.at[there], SQUARES, (at_z(k), j, at_x(dx, n)))
                        if (dx, k, n) == (0, 0, 1):
                            pl.when(y != j)(one.start)
                        else:
                            one.start()

        def send_out(k):
            send_squares(k, (2,))
            for j in (0, 2, 1, 3):
                one = remote(send_ag.at[0, pl.ds(3, 3)], from_ag.at[c], DIRECTION, (at_z(k), j, t))
                if k:
                    one.start()
                else:
                    pl.when(y != j)(one.start)
                remote(send_ag.at[0, pl.ds(0, 3)], from_ag.at[c], DIRECTION_0, (at_z(k), j, t0)).start()
            send_squares(k, (1, 3, 0))

        for first in (True, False):
            for k in (-2, 1, -1, 0):
                @pl.when((at_z(k) == 0) if first else (at_z(k) != 0))
                def _():
                    send_out(k)

        squares_o[there] = row
        from_ag[c] = direction[3:6]
        send_ag[1] = first_new
        send_ag[2] = second_new
        mom_o[0] = first_new[3:6]
        mom_o[1] = second_new[3:6]
        remote(send_ag.at[pl.ds(1, 2), pl.ds(0, 3)], mom_o, MOMENTS, (z, y, t0)).start()

        go_on(2)

        place(0)
        place(1)

        arrived(DIRECTION, from_ag.at[pl.ds(0, 15)])
        updates()
        place(2)

        arrived(SQUARES, squares_o.at[pl.ds(0, 63)])

        left(PART, from_y.at[pl.ds(0, 7)])
        left(CHUNK, from_z.at[pl.ds(0, 7)])
        left(DIRECTION, from_ag.at[pl.ds(0, 15)])
        left(DIRECTION_0, from_ag)
        left(MOMENTS, mom_o)
        left(OLD, old.at[pl.ds(0, 3)])
        weights_left()
        left(SQUARES, room)


def finish(
    uv, uq, wv, wq, mom, squares,
    uq_o, uv_o, wq_o, wv_o, fq_o, sq_o, fv_o, sv_o, cq_o, cv_o,
):
    z, y = lax.axis_index("fs"), lax.axis_index("rep")
    b = lax.div(z, 4)
    sums = [squares[k] for k in range(16 * X)]
    while len(sums) > 1:
        sums = [sums[k] + sums[k + 1] for k in range(0, len(sums), 2)]
    total = sums[0]
    query_lanes = iota((1, 128), 1) < 64
    sum_q = jnp.sum(jnp.where(query_lanes, total, 0.0), axis=1, keepdims=True)
    sum_v = jnp.sum(jnp.where(query_lanes, 0.0, total), axis=1, keepdims=True)
    scale_q = 1.0 / jnp.sqrt(sum_q / (RANK * QL * T) + 1.0)
    scale_v = 1.0 / jnp.sqrt(sum_v / (RANK * VL * T) + 1.0)

    half_q = (wq[:, 0:64] - 0.01 * (uq[...] * scale_q)).astype(BF16)
    same = one_hot(iota((QL, QL), 0) == iota((QL, QL), 1))
    cq_o[...] = nt(same, half_q).astype(BF16)
    cv_o[...] = (wv[...] - 0.01 * (uv[...] * scale_v)).astype(BF16)
    own = pl.multiple_of((z * Y + y) * ROWS, ROWS)
    update_q = uq[pl.ds(own, ROWS)] * scale_q
    update_v = uv[pl.ds(own, ROWS)] * scale_v
    uq_o[...] = update_q
    uv_o[...] = update_v
    wq_o[...] = wq[pl.ds(own, ROWS), 0:64] - 0.01 * update_q
    wv_o[...] = wv[pl.ds(own, ROWS)] - 0.01 * update_v

    for n, (q_out, v_out) in enumerate(((fq_o, fv_o), (sq_o, sv_o))):
        q_rows, v_rows = None, None
        for j in range(4):
            h, i = j // 2, 2 * (j % 2)
            v_now = mom[n, h, i : i + 2]
            q_now = mom[n, 2, i : i + 2, 64 * h : 64 * h + 64]
            q_rows = q_now if q_rows is None else jnp.where(b == j, q_now, q_rows)
            v_rows = v_now if v_rows is None else jnp.where(b == j, v_now, v_rows)
        q_out[...] = q_rows
        v_out[...] = v_rows


def body(x, cq, cv, bq, bv, wq, wv, fq, sq, fv, sv):
    anywhere = pl.BlockSpec(memory_space=pltpu.HBM)
    inside = pl.BlockSpec(memory_space=pltpu.VMEM)
    shape = jax.ShapeDtypeStruct
    dma = pltpu.SemaphoreType.DMA
    middle = pl.pallas_call(
        exchange,
        out_shape=(
            shape((D, VL), F32), shape((D, QL), F32), shape((D, VL), F32), shape((D, 128), F32),
            shape((2, 3, 4, 128), F32), shape((16 * X, 1, 128), F32),
        ),
        in_specs=[anywhere] * 11,
        out_specs=[inside] * 6,
        scratch_shapes=[
            pltpu.VMEM((128, D), BF16), pltpu.VMEM((QL, 256), BF16), pltpu.VMEM((256, VL), BF16),
            pltpu.VMEM((D, 256), BF16), pltpu.VMEM((ROWS, QL), F32), pltpu.VMEM((ROWS, VL), F32),
            pltpu.VMEM((2, 2, QL), F32), pltpu.VMEM((2, 2, VL), F32),
            pltpu.VMEM((Y, Z, 24, 128), F32),
            pltpu.VMEM((3, 2, 128), F32), pltpu.VMEM((4, 2, 3, 2, 128), F32),
            pltpu.VMEM((Y, 2, 24, 128), F32), pltpu.VMEM((4 * Y, 24, 128), F32),
            pltpu.VMEM((2, 6, 4, 128), F32), pltpu.VMEM((Z // 2, 6, 4, 128), F32),
            pltpu.VMEM((6, 4, 128), F32), pltpu.VMEM((6, 4, 128), F32),
            pltpu.VMEM((3, 6, 4, 128), F32), pltpu.VMEM((16, 3, 4, 128), F32),
            pltpu.VMEM((D, 256), BF16), pltpu.VMEM((D, 256), BF16),
            pltpu.VMEM((128, 128), F32), pltpu.VMEM((64, 128), F32), pltpu.VMEM((1, 128), F32),
            pltpu.VMEM((127, 1, 128), F32),
            dma((8,)), dma((KINDS,)), dma((KINDS,)),
            pltpu.SemaphoreType.REGULAR((2,)),
        ],
        compiler_params=pltpu.CompilerParams(collective_id=0, has_side_effects=True, vmem_limit_bytes=12 << 20),
        name="exchange",
    )(*(pltpu.with_memory_space_constraint(a, pltpu.HBM) for a in (x, cq.T, cv, bq, bv, wq, wv, fq, sq, fv, sv)))
    outs = pl.pallas_call(
        finish,
        out_shape=(
            shape((ROWS, QL), F32), shape((ROWS, VL), F32), shape((ROWS, QL), F32), shape((ROWS, VL), F32),
            shape((2, QL), F32), shape((2, QL), F32), shape((2, VL), F32), shape((2, VL), F32),
            shape((QL, D), BF16), shape((D, VL), BF16),
        ),
        in_specs=[inside] * 6,
        out_specs=[inside] * 10,
        compiler_params=pltpu.CompilerParams(vmem_limit_bytes=12 << 20),
        name="finish",
    )(*middle)
    return (*outs[:8], outs[8].T, outs[9])


def solution(mesh):
    rows = P(("fs", "rep"), "tp")
    in_specs = (P(("fs", "rep"), None), rows, rows, P(), P()) + (rows,) * 6
    out_specs = (rows,) * 8 + (P(None, "tp"),) * 2
    return jax.shard_map(body, mesh=mesh, in_specs=in_specs, out_specs=out_specs, check_vma=False)
```
